32 devices in a mesh: grp: 2 (over y), ep: 4 (over z), tp: 4 (over x, core).
Axes of the slice: x: 2, y: 2, z: 4, core: 2. Of those that a mesh axis runs over, the one named last changes fastest.
Arguments:
- hidden_in: bfloat16 [4096, 2048], P(('grp', 'ep', 'tp')), parts along dimension 0, may hold values from -6 to 6
- expert_ids: int32 [4096, 2], P(('grp', 'ep', 'tp')), parts along dimension 0, may hold values from 0 to 15, all different within a row; in each aligned block of 128 rows (0 to 127, 128 to 255, ...) at most 32 rows name the same one
- route_weights: float32 [4096, 2], P(('grp', 'ep', 'tp')), parts along dimension 0, may hold values from 0.1 to 1
- norm_gain: float32 [2048], replicated, may hold values from 0.1 to 1.9
- gate_proj: bfloat16 [16, 2048, 512], P(('ep', 'tp')), may hold values from -0.125 to 0.125
- up_proj: bfloat16 [16, 2048, 512], P(('ep', 'tp')), may hold values from -0.125 to 0.125
- down_proj: bfloat16 [16, 512, 2048], P(('ep', 'tp')), may hold values from -0.25 to 0.25
Outputs:
- mixed_out: bfloat16 [4096, 2048], P(('grp', 'ep', 'tp')), parts along dimension 0
The draws below stay inside these ranges and needn't reach their ends.
There are 2 independent parts, one for each index of `grp`. The reference program is written for one: setup_inputs(seed, part) draws one part's arguments, and reference() takes and returns one part's arrays. A program takes and returns all parts, laid end to end along the dimension named above; an argument that names none is the same for every part. Nothing has to cross between parts.
Inputs may be any that keep to these rules, and one draw needn't show every extreme that they name: `expert_ids`: each token names 2 different experts; among the 128 tokens of one device (aligned blocks of rows) no expert is named more than 32 times, and in every draw some expert is named exactly 32 times by some device's tokens.
All inputs are finite; a program needn't handle non-finite values.
Results may differ from the reference program's by a relative error of at most 0.0071.
Values may be sent and summed in bfloat16 or wider, within the bound.
A program may use at most 64 MiB of HBM per device.

```python
import math
import jax
import jax.numpy as jnp
import numpy as np
from jax import lax

D = 2048
FE = 512
TOP_K = 2
TOK_DEV = 128
EXPERTS = 16
TOKENS = 2048
CAP = 32
N_EP = 4
N_TP = 4


def block_levels(stream_key, shape, cuts, least, high):
    gain, own = 1.0, jax.random.fold_in(stream_key, 6)
    for dim, blocks in cuts:
        steps = jnp.exp(jax.random.uniform(jax.random.fold_in(own, dim), (blocks,), jnp.float32, least / len(cuts), high / len(cuts)))
        gain = gain * jnp.repeat(steps, shape[dim] // blocks).reshape([-1 if axis == dim else 1 for axis in range(len(shape))])
    return gain


def shared_out(key, own, number, rows, amount, top, reach, lean):
    ranking = jax.random.permutation(key, amount)
    packed, ordinary = portions_of(amount, rows * top, reach, lean, True), portions_of(amount, rows * top, reach, lean, False)
    places = jnp.arange(amount)

    def named(lengths, offset_by):
        used = int((lengths > 0).sum())
        fixed = max(1, used // 4)
        passed = fixed + (places - fixed + offset_by * (used - fixed)) % max(1, amount - fixed)
        return jnp.zeros((amount,), jnp.int32).at[ranking[jnp.where(places < fixed, places, passed)]].set(jnp.asarray(lengths, jnp.int32))

    lengths = jnp.where(number % 4 == 0, named(packed, number // 4), named(ordinary, number - number // 4 - 1))
    mixed = jax.random.permutation(jax.random.fold_in(own, 3), amount)
    donor, taker = mixed[0:amount // 2 * 2:2], mixed[1:amount // 2 * 2:2]
    room = jnp.minimum(lengths[donor] - 1, reach - lengths[taker]) // 2
    room = jnp.where((donor == ranking[0]) | (taker == ranking[0]) | (lengths[taker] == 0), 0, jnp.maximum(room, 0))
    passed = jax.random.randint(jax.random.fold_in(own, 4), (amount // 2,), 0, 1 << 20) % (room + 1)
    lengths = lengths.at[donor].add(-passed).at[taker].add(passed)
    labels = jnp.searchsorted(jnp.cumsum(lengths), jnp.arange(rows * top), side="right").astype(jnp.int32)
    listing = labels.reshape(top, rows).T
    listing = listing[jax.random.permutation(jax.random.fold_in(own, 1), rows)]
    offset_by = jax.random.randint(jax.random.fold_in(own, 2), (rows, 1), 0, top)
    return jnp.take_along_axis(listing, (jnp.arange(top)[None, :] + offset_by) % top, axis=1)


def portions_of(amount, total, most, lean, full):
    weights = [(1 << 20) // math.isqrt(rank ** lean) + 1 for rank in range(1, amount + 1)]
    largest = most if full else min(most, max(-(-total // amount), total * weights[0] // sum(weights)))
    least = 1 if total - largest >= amount - 1 else 0
    given, surplus = [largest] + [least] * (amount - 1), total - largest - least * (amount - 1)
    while surplus > 0:
        free = [i for i in range(1, amount) if given[i] < largest] or [i for i in range(1, amount) if given[i] < most]
        mass, remaining = sum([weights[i] for i in free]), surplus
        for i in free:
            addition = min(most - given[i], max(1, remaining * weights[i] // mass), surplus)
            given[i] = given[i] + addition
            surplus = surplus - addition
    return np.array(given)


def gaussian(stream_key, extent, deviation, most, split=(), held_as=jnp.bfloat16):
    result = jax.random.normal(stream_key, extent, jnp.float32) * deviation
    if len(split) > 0:
        result = block_levels(stream_key, extent, split, -0.22, 0.18) * result
    return jnp.clip(result, min=-most, max=most).astype(held_as)


def setup_inputs(seed: int = 0, part: int = 0) -> dict:
    splits = jax.random.split(jax.random.key(seed), 8)
    own_keys = jax.random.split(jax.random.fold_in(splits[7], part), 8)
    hidden_in = gaussian(own_keys[0], (TOKENS, D), 1.0, 6.0, ((0, 16),))
    expert_ids_keys = jax.random.split(jax.random.fold_in(own_keys[1], 1), TOKENS // TOK_DEV)
    expert_ids_turns = jax.random.permutation(jax.random.fold_in(own_keys[1], 3), TOKENS // TOK_DEV)
    expert_ids = jax.vmap(lambda own, number: shared_out(jax.random.fold_in(own_keys[1], 2), own, number, TOK_DEV, EXPERTS, TOP_K, CAP, 2))(expert_ids_keys, expert_ids_turns).reshape((TOKENS, TOP_K))
    route_weights = jnp.clip(jnp.exp(math.log(1.0) - 2.3025851 * jax.random.uniform(own_keys[2], (TOKENS, TOP_K), jnp.float32) ** block_levels(own_keys[2], (TOKENS, TOP_K), ((0, 16),), -0.2, 0.2)), 0.1, 1.0)
    norm_gain = jnp.clip(1.0 + 0.18 * jax.random.normal(splits[3], (D,), jnp.float32), 0.1, 1.9)
    gate_proj = gaussian(splits[4], (EXPERTS, D, FE), D ** -0.5, 0.125, ((0, 16),))
    up_proj = gaussian(splits[5], (EXPERTS, D, FE), D ** -0.5, 0.125, ((0, 16),))
    down_proj = gaussian(splits[6], (EXPERTS, FE, D), FE ** -0.5, 0.25, ((0, 16),))
    return dict(hidden_in=hidden_in, expert_ids=expert_ids, route_weights=route_weights, norm_gain=norm_gain, gate_proj=gate_proj, up_proj=up_proj, down_proj=down_proj)


def reference(hidden_in, expert_ids, route_weights, norm_gain, gate_proj, up_proj, down_proj):
    device_count = N_EP * N_TP
    as_float = hidden_in.astype(jnp.float32)
    scaled = as_float * lax.rsqrt(lax.optimization_barrier(jnp.mean(as_float * as_float, axis=-1, keepdims=True)) + 1e-06)
    normed = (scaled * norm_gain).astype(jnp.bfloat16)
    flat_ids = expert_ids.reshape(device_count, TOK_DEV * TOP_K).astype(jnp.int32)
    onehot = (flat_ids[:, :, None] == jnp.arange(EXPERTS, dtype=jnp.int32)[None, None, :]).astype(jnp.int32)
    slot_index = lax.optimization_barrier(jnp.sum((jnp.cumsum(onehot, axis=1) - onehot) * onehot, axis=2)).astype(jnp.int32)
    source = jnp.arange(device_count, dtype=jnp.int32)[:, None]
    target = (flat_ids * (device_count * CAP) + source * CAP + slot_index).reshape(-1).astype(jnp.int32)
    routed = jnp.repeat(normed, TOP_K, axis=0)
    expert_rows = jnp.zeros((EXPERTS * device_count * CAP, D), jnp.bfloat16).at[target].set(routed)
    expert_rows = expert_rows.reshape(EXPERTS, device_count * CAP, D)

    def run_expert(pieces):
        block_in, weight_gate, weight_up, weight_down = pieces
        block_float = block_in.astype(jnp.float32)
        gate_act = jnp.dot(block_float, weight_gate.astype(jnp.float32))
        up_act = jnp.dot(block_float, weight_up.astype(jnp.float32))
        hidden = (jax.nn.silu(gate_act) * up_act).astype(jnp.bfloat16)
        return jnp.dot(hidden.astype(jnp.float32), weight_down.astype(jnp.float32)).astype(jnp.bfloat16)
    expert_out = lax.map(run_expert, (expert_rows, gate_proj, up_proj, down_proj))
    picked = expert_out.reshape(-1, D)[target].astype(jnp.float32).reshape(TOKENS, TOP_K, D)
    return lax.optimization_barrier(jnp.sum(picked * route_weights[:, :, None], axis=1)).astype(jnp.bfloat16)
```

```python
import functools

import jax
import jax.numpy as jnp
from jax import lax
from jax.experimental import pallas as pl
from jax.experimental.pallas import tpu as pltpu
from jax.sharding import PartitionSpec as P

CHUNKS = 4
OWN, OUTER, INNER, FAR = 0, 1, 2, 3


def slot_capacity(choose_count, token_count, expert_count):
    return max(2, 2 * choose_count * token_count // expert_count)


def kernel(
    n, m, cap, chunks,
    hid_hbm, ids_hbm, wts_hbm, gain_hbm, gate_hbm, up_hbm, down_hbm, out,
    hid, ids, wts, gain, gate, up, down,
    tok, meta, mixes, dsp, dse, xin, res, back, esl, part, rin, acc, pre,
    in_sem, ag_s, ag_r, me_s, me_r, xd_s, xd_r, de_s, xb_s, xb_r, es_s, es_r, rs_s, rs_r,
):
    z = lax.axis_index("ep")
    t = lax.axis_index("tp")
    tokens, width = hid.shape
    rows = m * cap
    cw = width // chunks
    choose = ids.shape[0]
    experts = n * m
    middle = jnp.logical_and(z > 0, z < n - 1)
    end = jnp.logical_or(z == 0, z == n - 1)
    inner = n - 1 - z
    outer = jnp.where(z <= 1, 0, n - 1)
    near = jnp.where(z == 0, 1, n - 2)

    def cols(c):
        return pl.ds(c * cw, cw)

    loads = [
        pltpu.make_async_copy(src, dst, in_sem.at[i])
        for i, (src, dst) in enumerate([
            (hid_hbm, hid), (ids_hbm, ids), (wts_hbm, wts), (gain_hbm, gain),
            (gate_hbm.at[0], gate), (up_hbm.at[0], up), (down_hbm.at[0], down),
        ])
    ]
    for load in loads:
        load.start()

    barrier = pltpu.get_barrier_semaphore()

    def greet(dev):
        pl.semaphore_signal(
            barrier, inc=1, device_id=dev, device_id_type=pl.DeviceIdType.MESH
        )

    for d in range(1, m):
        greet({"tp": lax.rem(t + d, m)})

    @pl.when(middle)
    def _():
        greet({"ep": inner})
        for j in range(m):
            greet({"ep": outer, "tp": jnp.int32(j)})

    @pl.when(end)
    def _():
        for j in range(m):
            greet({"ep": near, "tp": jnp.int32(j)})

    def remote(src, dst, s_sem, r_sem, dev):
        return pltpu.make_async_remote_copy(
            src_ref=src, dst_ref=dst, send_sem=s_sem, recv_sem=r_sem,
            device_id=dev, device_id_type=pl.DeviceIdType.MESH,
        )

    def ag_copy(src, dst, slot, c, dev):
        return remote(tok.at[src, c], tok.at[dst, c], ag_s.at[slot, c], ag_r.at[dst, c], dev)

    def me_copy(src, dst, slot, dev):
        return remote(meta.at[src], meta.at[dst], me_s.at[slot], me_r.at[dst], dev)

    def xd_copy(r, j, c):
        return remote(
            dsp.at[r, c, j], xin.at[r, c, t], xd_s.at[r, j, c], xd_r.at[r, t, c], {"tp": j}
        )

    def xd_from(r, j, c):
        return remote(
            dsp.at[r, c, j], xin.at[r, c, j], xd_s.at[r, j, c], xd_r.at[r, j, c], {"tp": j}
        )

    def de_copy(i, j, c):
        return remote(
            dse.at[i, c, j], xin.at[i + 1, c, t], de_s.at[i, j, c], xd_r.at[i + 1, t, c],
            {"ep": outer, "tp": jnp.int32(j)},
        )

    def xb_copy(r, j, c):
        return remote(
            res.at[r, c, j], back.at[r, c, t], xb_s.at[r, j, c], xb_r.at[r, t, c], {"tp": j}
        )

    def xb_from(r, j, c):
        return remote(
            res.at[r, c, j], back.at[r, c, j], xb_s.at[r, j, c], xb_r.at[r, j, c], {"tp": j}
        )

    def es_copy(i, c):
        return remote(back.at[i + 1, c], esl.at[i, c], es_s.at[i, c], es_r.at[i, c], {"ep": near})

    def rs_copy(i, k, c, dev):
        return remote(part.at[i, c], rin.at[k, c], rs_s.at[i, c], rs_r.at[k, c], dev)

    def peers():
        return [lax.rem(t + d, m) for d in range(m - 1, 0, -1)]

    loads[1].wait()
    loads[2].wait()
    expert_row = lax.broadcasted_iota(jnp.int32, (experts, tokens), 0)
    named = [(expert_row == ids[k : k + 1, :]).astype(jnp.float32) for k in range(choose)]
    total = named[0]
    for k in range(1, choose):
        total = total + named[k]
    before = (
        lax.broadcasted_iota(jnp.int32, (tokens, tokens), 0)
        < lax.broadcasted_iota(jnp.int32, (tokens, tokens), 1)
    ).astype(jnp.bfloat16)
    counts = jnp.dot(total.astype(jnp.bfloat16), before, preferred_element_type=jnp.float32)
    first = expert_row.astype(jnp.float32) * cap + counts
    lines = [jnp.sum(named[k] * first, axis=0, keepdims=True) for k in range(choose)]
    lines += [wts[k : k + 1, :] for k in range(choose)]
    lines.append(jnp.zeros((meta.shape[1] - 2 * choose, tokens), jnp.float32))
    meta[OWN] = jnp.concatenate(lines, axis=0)

    loads[0].wait()
    loads[3].wait()
    hidden = hid[...].astype(jnp.float32)
    scale = lax.rsqrt(jnp.mean(hidden * hidden, axis=-1, keepdims=True) + 1e-06)
    for c in range(chunks):
        normed = hidden[:, c * cw : (c + 1) * cw] * scale * gain[:, cols(c)]
        tok[OWN, c] = normed.astype(jnp.bfloat16)

    def slot_rows(sides):
        parts = [
            lax.broadcasted_iota(jnp.int32, (rows, tokens), 0) + side * rows for side in sides
        ]
        return jnp.concatenate(parts, axis=0).astype(jnp.float32)

    def selection(r, sides):
        info = meta[r]
        row = slot_rows(sides)
        select = jnp.zeros(row.shape, jnp.float32)
        for k in range(choose):
            select = select + (row == info[k : k + 1, :]).astype(jnp.float32)
        return select.astype(jnp.bfloat16)

    def mixing(r, sides):
        info = meta[r]
        row = slot_rows(sides)
        mix = jnp.zeros(row.shape, jnp.float32)
        for k in range(choose):
            mix = mix + jnp.where(
                row == info[k : k + 1, :], info[choose + k : choose + k + 1, :], 0.0
            )
        mixes[r, :, 0 : len(sides) * rows] = jnp.transpose(mix).astype(jnp.bfloat16)

    def dispatch(r, c, select, split):
        sent = jnp.dot(select, tok[r, c], preferred_element_type=jnp.float32).astype(jnp.bfloat16)
        if split:
            i = 0 if r == OWN else r - 1
            dse[i, c] = sent[rows:, :].reshape(m, cap, cw)
            for j in range(m):
                de_copy(i, j, c).start()
        dsp[r, c] = sent[0:rows, :].reshape(m, cap, cw)
        for j in peers():
            xd_copy(r, j, c).start()
        xin[r, c, t] = dsp[r, c, t]

    def experts_step(r, direct):
        if r == (1 if direct else INNER):
            loads[4].wait()
            loads[5].wait()
        gate_act = jnp.zeros((rows, gate.shape[1]), jnp.float32)
        up_act = jnp.zeros((rows, gate.shape[1]), jnp.float32)
        for c in range(chunks):
            for j in ([jnp.int32(j) for j in range(m)] if direct else peers()):
                xd_from(r, j, c).wait_recv()
            block = xin[r, c].reshape(rows, cw)
            gate_act += jnp.dot(block, gate[cols(c), :], preferred_element_type=jnp.float32)
            up_act += jnp.dot(block, up[cols(c), :], preferred_element_type=jnp.float32)
        act = (gate_act / (1.0 + jnp.exp(-gate_act)) * up_act).astype(jnp.bfloat16)
        if r == (1 if direct else INNER):
            loads[6].wait()
        for c in range(chunks):
            made = jnp.dot(act, down[:, cols(c)], preferred_element_type=jnp.float32)
            res[r, c] = made.astype(jnp.bfloat16).reshape(m, cap, cw)
            for j in peers():
                xb_copy(r, j, c).start()
            back[r, c, t] = res[r, c, t]

    def returned(r, c):
        for j in peers():
            xb_from(r, j, c).wait_recv()

    def combined(r, c, i):
        value = jnp.dot(
            mixes[r, :, 0:rows], back[r, c].reshape(rows, cw), preferred_element_type=jnp.float32
        )
        if i is not None:
            value = value + jnp.dot(
                mixes[r, :, rows : 2 * rows], esl[i, c].reshape(rows, cw),
                preferred_element_type=jnp.float32,
            )
        return value

    @pl.when(middle)
    def _():
        pl.semaphore_wait(barrier, 2 * m)
        to_in, to_out = {"ep": inner}, {"ep": outer}
        me_copy(OWN, INNER, 0, to_in).start()
        for c in range(chunks):
            ag_copy(OWN, INNER, 0, c, to_in).start()
        sides = [z, outer]
        select = selection(OWN, sides)
        for c in range(chunks):
            dispatch(OWN, c, select, True)
        mixing(OWN, sides)

        sel_o = sel_i = None
        for c in range(chunks):
            if c == 0:
                me_copy(OWN, OUTER, 0, to_in).wait_recv()
                me_copy(OUTER, FAR, 1, to_in).start()
                sel_o = selection(OUTER, [z])
            ag_copy(OWN, OUTER, 0, c, to_in).wait_recv()
            ag_copy(OUTER, FAR, 1, c, to_in).start()
            if c == 0:
                me_copy(OWN, INNER, 0, to_in).wait_recv()
                sel_i = selection(INNER, sides)
            ag_copy(OWN, INNER, 0, c, to_in).wait_recv()
            dispatch(INNER, c, sel_i, True)
            dispatch(OUTER, c, sel_o, False)
        mixing(OUTER, [z])
        mixing(INNER, sides)

        me_copy(OUTER, FAR, 1, to_in).wait_recv()
        sel_f = selection(FAR, sides)
        for c in range(chunks):
            ag_copy(OUTER, FAR, 1, c, to_in).wait_recv()
            dispatch(FAR, c, sel_f, True)
            if c == 0:
                experts_step(INNER, False)
        mixing(FAR, sides)
        experts_step(FAR, False)
        experts_step(OUTER, False)
        experts_step(OWN, False)

        def to_inner(i, r, e, c):
            returned(r, c)
            es_copy(e, c).wait_recv()
            part[i, c] = combined(r, c, e).astype(jnp.bfloat16)
            rs_copy(i, i, c, to_in).start()

        def to_outer(c):
            rs_copy(1, 1, c, to_in).wait_recv()
            part[2, c] = (pre[c] + rin[1, c].astype(jnp.float32)).astype(jnp.bfloat16)
            rs_copy(2, 0, c, to_out).start()

        for c in range(chunks):
            to_inner(0, INNER, 1, c)
        for c in range(chunks):
            returned(OUTER, c)
            pre[c] = combined(OUTER, c, None)
        for c in range(chunks):
            returned(OWN, c)
            es_copy(0, c).wait_recv()
            acc[:, cols(c)] = combined(OWN, c, 0)
        lag = 2
        for c in range(chunks + lag):
            if c < chunks:
                to_inner(1, FAR, 2, c)
                rs_copy(0, 0, c, to_in).wait_recv()
                value = acc[:, cols(c)] + rin[0, c].astype(jnp.float32)
                out[:, cols(c)] = value.astype(jnp.bfloat16)
            if c >= lag:
                to_outer(c - lag)

        for s in range(2):
            me_copy(OWN, INNER, s, to_in).wait_send()
            for c in range(chunks):
                ag_copy(OWN, INNER, s, c, to_in).wait_send()
        for c in range(chunks):
            for j in range(m):
                for i in range(3):
                    de_copy(i, j, c).wait_send()
            for r in range(4):
                for j in peers():
                    xd_copy(r, j, c).wait_send()
                    xb_copy(r, j, c).wait_send()
            for i in range(3):
                rs_copy(i, 0, c, to_in).wait_send()

    @pl.when(end)
    def _():
        pl.semaphore_wait(barrier, 2 * m - 1)
        to_near = {"ep": near}
        me_copy(OWN, OUTER, 0, to_near).start()
        for c in range(chunks):
            ag_copy(OWN, OUTER, 0, c, to_near).start()
        select = selection(OWN, [z])
        for c in range(chunks):
            dispatch(OWN, c, select, False)
        mixing(OWN, [z])
        for r in range(1, 4):
            experts_step(r, True)
            for c in range(chunks):
                returned(r, c)
                es_copy(r - 1, c).start()
        experts_step(OWN, False)
        for c in range(chunks):
            returned(OWN, c)
            acc[:, cols(c)] = combined(OWN, c, None)
        for c in range(chunks):
            rs_copy(2, 0, c, to_near).wait_recv()
            value = acc[:, cols(c)] + rin[0, c].astype(jnp.float32)
            out[:, cols(c)] = value.astype(jnp.bfloat16)

        me_copy(OWN, OUTER, 0, to_near).wait_send()
        for c in range(chunks):
            ag_copy(OWN, OUTER, 0, c, to_near).wait_send()
            for j in peers():
                xd_copy(OWN, j, c).wait_send()
                for r in range(4):
                    xb_copy(r, j, c).wait_send()
            for i in range(3):
                es_copy(i, c).wait_send()


def fused(n, m, cap, hidden_in, expert_ids, route_weights, norm_gain, gate_proj, up_proj, down_proj):
    tokens, width = hidden_in.shape
    units = gate_proj.shape[2]
    chunks = CHUNKS
    cw = width // chunks
    choose = expert_ids.shape[1]
    lines = -(-2 * choose // 8) * 8
    bf, f32 = jnp.bfloat16, jnp.float32
    dma = pltpu.SemaphoreType.DMA
    hbm = pl.BlockSpec(memory_space=pl.ANY)
    slots = lambda k: pltpu.VMEM((k, chunks, m, cap, cw), bf)
    block = lambda k: pltpu.VMEM((k, chunks, tokens, cw), bf)
    return pl.pallas_call(
        functools.partial(kernel, n, m, cap, chunks),
        out_shape=jax.ShapeDtypeStruct((tokens, width), bf),
        in_specs=[hbm] * 7,
        out_specs=pl.BlockSpec(memory_space=pltpu.VMEM),
        scratch_shapes=[
            pltpu.VMEM((tokens, width), bf),
            pltpu.VMEM((choose, tokens), jnp.int32),
            pltpu.VMEM((choose, tokens), f32),
            pltpu.VMEM((1, width), f32),
            pltpu.VMEM((width, units), bf),
            pltpu.VMEM((width, units), bf),
            pltpu.VMEM((units, width), bf),
            block(4),
            pltpu.VMEM((4, lines, tokens), f32),
            pltpu.VMEM((4, tokens, 2 * m * cap), bf),
            slots(4), slots(3), slots(4), slots(4), slots(4), slots(3),
            block(3), block(2),
            pltpu.VMEM((tokens, width), f32),
            pltpu.VMEM((chunks, tokens, cw), f32),
            dma((7,)),
            dma((2, chunks)), dma((4, chunks)),
            dma((2,)), dma((4,)),
            dma((4, m, chunks)), dma((4, m, chunks)), dma((3, m, chunks)),
            dma((4, m, chunks)), dma((4, m, chunks)),
            dma((3, chunks)), dma((3, chunks)),
            dma((3, chunks)), dma((2, chunks)),
        ],
        compiler_params=pltpu.CompilerParams(
            collective_id=0, has_side_effects=True, vmem_limit_bytes=60 * 1024 * 1024
        ),
        name="experts",
    )(
        hidden_in, expert_ids.T, route_weights.T, norm_gain.reshape(1, -1),
        gate_proj, up_proj, down_proj,
    )


def by_slots(capacity, hidden_in, expert_ids, route_weights, norm_gain, gate_proj, up_proj, down_proj):
    token_count = hidden_in.shape[0]
    model_width = hidden_in.shape[1]
    choose_count = expert_ids.shape[1]
    expert_count = lax.axis_size("ep") * lax.axis_size("tp")
    as_float = hidden_in.astype(jnp.float32)
    scaled = as_float * lax.rsqrt(jnp.mean(as_float * as_float, axis=-1, keepdims=True) + 1e-06)
    normed = (scaled * norm_gain).astype(jnp.bfloat16)
    flat_ids = expert_ids.reshape(-1)
    onehot = (flat_ids[:, None] == jnp.arange(expert_count, dtype=jnp.int32)[None, :]).astype(
        jnp.int32
    )
    slot_index = jnp.sum((jnp.cumsum(onehot, axis=0) - onehot) * onehot, axis=1)
    target = flat_ids * capacity + slot_index
    routed = jnp.repeat(normed, choose_count, axis=0)
    buffer = jnp.zeros((expert_count * capacity, model_width), jnp.bfloat16).at[target].set(routed)
    buffer = buffer.reshape(expert_count, capacity, model_width)
    arrived = lax.all_to_all(buffer, ("ep", "tp"), split_axis=0, concat_axis=0, tiled=True)
    shape_in = arrived.shape
    block_in = arrived.reshape(-1, model_width)
    gate_act = jnp.dot(block_in, gate_proj[0], preferred_element_type=jnp.float32)
    up_act = jnp.dot(block_in, up_proj[0], preferred_element_type=jnp.float32)
    hidden = (jax.nn.silu(gate_act) * up_act).astype(jnp.bfloat16)
    result = jnp.dot(hidden, down_proj[0], preferred_element_type=jnp.float32).astype(jnp.bfloat16)
    results = result.reshape(shape_in)
    returned = lax.all_to_all(results, ("ep", "tp"), split_axis=0, concat_axis=0, tiled=True)
    picked = returned.reshape(-1, model_width)[target].astype(jnp.float32)
    picked = picked.reshape(token_count, choose_count, model_width)
    return jnp.sum(picked * route_weights[:, :, None], axis=1).astype(jnp.bfloat16)


def body(hidden_in, expert_ids, *rest):
    n, m = lax.axis_size("ep"), lax.axis_size("tp")
    tokens = hidden_in.shape[0]
    cap = slot_capacity(expert_ids.shape[1], tokens, n * m)
    if n == 4 and m * cap >= tokens and cap % 16 == 0:
        return fused(n, m, cap, hidden_in, expert_ids, *rest)
    return by_slots(cap, hidden_in, expert_ids, *rest)


def solution(mesh):
    return jax.shard_map(
        body,
        mesh=mesh,
        in_specs=(
            P(("grp", "ep", "tp"), None),
            P(("grp", "ep", "tp"), None),
            P(("grp", "ep", "tp"), None),
            P(),
            P(("ep", "tp"), None, None),
            P(("ep", "tp"), None, None),
            P(("ep", "tp"), None, None),
        ),
        out_specs=P(("grp", "ep", "tp"), None),
        check_vma=False,
    )
```

```python
import functools

import jax
import jax.numpy as jnp
from jax import lax
from jax.experimental import pallas as pl
from jax.experimental.pallas import tpu as pltpu
from jax.sharding import PartitionSpec as P

CHUNKS = 4
BACK_CHUNKS = 8
OWN, OUTER, INNER, FAR = 0, 1, 2, 3


def slot_capacity(choose_count, token_count, expert_count):
    return max(2, 2 * choose_count * token_count // expert_count)


def kernel(
    n, m, cap, chunks, bchunks,
    hid_hbm, ids_hbm, wts_hbm, gain_hbm, gate_hbm, up_hbm, down_hbm, out,
    hid, ids, wts, gain, gate, up, down,
    tok, meta, mixes, dsp, dse, xin, res, back, esl, part, rin, pre,
    in_sem, ag_s, ag_r, me_s, me_r, xd_s, xd_r, de_s, xb_s, xb_r, es_s, es_r, rs_s, rs_r,
):
    z = lax.axis_index("ep")
    t = lax.axis_index("tp")
    tokens, width = hid.shape
    rows = m * cap
    cw = width // chunks
    bw = width // bchunks
    half = cap // 2
    choose = ids.shape[0]
    experts = n * m
    middle = jnp.logical_and(z > 0, z < n - 1)
    end = jnp.logical_or(z == 0, z == n - 1)
    inner = n - 1 - z
    outer = jnp.where(z <= 1, 0, n - 1)
    near = jnp.where(z == 0, 1, n - 2)

    def cols(c):
        return pl.ds(c * cw, cw)

    def bcols(c):
        return pl.ds(c * bw, bw)

    loads = [
        pltpu.make_async_copy(src, dst, in_sem.at[i])
        for i, (src, dst) in enumerate([
            (hid_hbm, hid), (ids_hbm, ids), (wts_hbm, wts), (gain_hbm, gain),
            (gate_hbm.at[0], gate), (up_hbm.at[0], up), (down_hbm.at[0], down),
        ])
    ]
    for load in loads:
        load.start()

    barrier = pltpu.get_barrier_semaphore()

    def greet(dev):
        pl.semaphore_signal(
            barrier, inc=1, device_id=dev, device_id_type=pl.DeviceIdType.MESH
        )

    for d in range(1, m):
        greet({"tp": lax.rem(t + d, m)})

    @pl.when(middle)
    def _():
        greet({"ep": inner})
        for j in range(m):
            greet({"ep": outer, "tp": jnp.int32(j)})

    @pl.when(end)
    def _():
        for j in range(m):
            greet({"ep": near, "tp": jnp.int32(j)})

    def remote(src, dst, s_sem, r_sem, dev):
        return pltpu.make_async_remote_copy(
            src_ref=src, dst_ref=dst, send_sem=s_sem, recv_sem=r_sem,
            device_id=dev, device_id_type=pl.DeviceIdType.MESH,
        )

    def lot(r):
        return r, r, 0, cap

    first_half, second_half = (1, 1, 0, half), (4, 1, half, cap - half)
    others, self_id = pl.ds(0, m - 1), {"tp": t}

    def ag_copy(src, dst, slot, c, dev):
        return remote(tok.at[src, c], tok.at[dst, c], ag_s.at[slot], ag_r.at[dst, c], dev)

    def ag_sent(slot):
        remote(tok.at[0], tok.at[0], ag_s.at[slot], ag_r.at[0, 0], self_id).wait_send()

    def me_copy(src, dst, slot, dev):
        return remote(meta.at[src], meta.at[dst], me_s.at[slot], me_r.at[dst], dev)

    def xd_copy(r, j, c):
        return remote(
            dsp.at[r, c, j], xin.at[r, c, t], xd_s.at[r], xd_r.at[r, c], {"tp": j}
        )

    def xd_from(r, c):
        return remote(
            dsp.at[r, c, others], xin.at[r, c, others], xd_s.at[r], xd_r.at[r, c], self_id
        )

    def xd_sent(r):
        remote(
            dsp.at[r, :, others], xin.at[r, :, others], xd_s.at[r], xd_r.at[r, 0], self_id
        ).wait_send()

    def spread():
        return [lax.rem(t + lax.rem(t, 2) + d, m) for d in range(m)]

    def de_copy(part_of, j, c):
        k, r, lo, size = part_of
        here = pl.ds(lo, size)
        return remote(
            dse.at[r - 1, c, j, here], xin.at[r, c, t, here], de_s.at[k - 1],
            xd_r.at[k, c], {"ep": outer, "tp": j},
        )

    def de_from(part_of, c):
        k, r, lo, size = part_of
        here = pl.ds(lo, size)
        return remote(
            dse.at[r - 1, c, :, here], xin.at[r, c, :, here], de_s.at[k - 1],
            xd_r.at[k, c], self_id,
        )

    def de_sent(part_of):
        k, r, lo, size = part_of
        here = pl.ds(lo, size)
        remote(
            dse.at[r - 1, :, :, here], xin.at[r, :, :, here], de_s.at[k - 1],
            xd_r.at[k, 0], self_id,
        ).wait_send()

    def xb_copy(part_of, j, c):
        k, r, lo, size = part_of
        here = pl.ds(lo, size)
        return remote(
            res.at[r, c, j, here], back.at[r, c, t, here], xb_s.at[k],
            xb_r.at[k, c], {"tp": j},
        )

    def xb_from(part_of, c):
        k, r, lo, size = part_of
        here = pl.ds(lo, size)
        return remote(
            res.at[r, c, others, here], back.at[r, c, others, here], xb_s.at[k],
            xb_r.at[k, c], self_id,
        )

    def xb_sent(part_of):
        k, r, lo, size = part_of
        here = pl.ds(lo, size)
        remote(
            res.at[r, :, others, here], back.at[r, :, others, here], xb_s.at[k],
            xb_r.at[k, 0], self_id,
        ).wait_send()

    def es_copy(part_of, c):
        k, r, lo, size = part_of
        here = pl.ds(lo, size)
        return remote(
            back.at[r, c, :, here], esl.at[r - 1, c, :, here], es_s.at[k - 1],
            es_r.at[k - 1, c], {"ep": near},
        )

    def es_sent(part_of):
        k, r, lo, size = part_of
        here = pl.ds(lo, size)
        remote(
            back.at[r, :, :, here], esl.at[r - 1, :, :, here], es_s.at[k - 1],
            es_r.at[k - 1, 0], self_id,
        ).wait_send()

    def rs_copy(i, k, c, dev):
        return remote(part.at[i, c], rin.at[k, c], rs_s.at[i], rs_r.at[k, c], dev)

    def rs_sent(i):
        remote(part.at[i], rin.at[0], rs_s.at[i], rs_r.at[0, 0], self_id).wait_send()

    def peers():
        return [lax.rem(t + d, m) for d in range(m - 1, 0, -1)]

    loads[1].wait()
    loads[2].wait()
    expert_row = lax.broadcasted_iota(jnp.int32, (experts, tokens), 0)
    named = [(expert_row == ids[k : k + 1, :]).astype(jnp.float32) for k in range(choose)]
    total = named[0]
    for k in range(1, choose):
        total = total + named[k]
    before = (
        lax.broadcasted_iota(jnp.int32, (tokens, tokens), 0)
        < lax.broadcasted_iota(jnp.int32, (tokens, tokens), 1)
    ).astype(jnp.bfloat16)
    counts = jnp.dot(total.astype(jnp.bfloat16), before, preferred_element_type=jnp.float32)
    first = expert_row.astype(jnp.float32) * cap + counts
    lines = [jnp.sum(named[k] * first, axis=0, keepdims=True) for k in range(choose)]
    lines += [wts[k : k + 1, :] for k in range(choose)]
    lines.append(jnp.zeros((meta.shape[1] - 2 * choose, tokens), jnp.float32))
    meta[OWN] = jnp.concatenate(lines, axis=0)

    loads[0].wait()
    loads[3].wait()
    hidden = hid[...].astype(jnp.float32)
    scale = lax.rsqrt(jnp.mean(hidden * hidden, axis=-1, keepdims=True) + 1e-06)
    for c in range(chunks):
        normed = hidden[:, c * cw : (c + 1) * cw] * scale * gain[:, cols(c)]
        tok[OWN, c] = normed.astype(jnp.bfloat16)

    def slot_rows(sides):
        parts = [
            lax.broadcasted_iota(jnp.int32, (rows, tokens), 0) + side * rows for side in sides
        ]
        return jnp.concatenate(parts, axis=0).astype(jnp.float32)

    def selection(r, sides):
        info = meta[r]
        row = slot_rows(sides)
        select = jnp.zeros(row.shape, jnp.float32)
        for k in range(choose):
            select = select + (row == info[k : k + 1, :]).astype(jnp.float32)
        return select.astype(jnp.bfloat16)

    def mixing(r, sides):
        info = meta[r]
        row = slot_rows(sides)
        mix = jnp.zeros(row.shape, jnp.float32)
        for k in range(choose):
            mix = mix + jnp.where(
                row == info[k : k + 1, :], info[choose + k : choose + k + 1, :], 0.0
            )
        mixes[r, :, 0 : len(sides) * rows] = jnp.transpose(mix).astype(jnp.bfloat16)

    def dispatch(r, c, select):
        sent = jnp.dot(select, tok[r, c], preferred_element_type=jnp.float32).astype(jnp.bfloat16)
        if select.shape[0] > rows:
            i = 0 if r == OWN else r - 1
            dse[i, c] = sent[rows:, :].reshape(m, cap, cw)
            for j in spread():
                de_copy(first_half if r == OWN else lot(r), j, c).start()
        dsp[r, c] = sent[0:rows, :].reshape(m, cap, cw)
        for j in peers():
            xd_copy(r, j, c).start()
        xin[r, c, t] = dsp[r, c, t]

    def experts_step(part_of, direct, opening=False, send=True):
        k, r, lo, size = part_of
        if opening:
            loads[4].wait()
            loads[5].wait()
        gate_act = jnp.zeros((m * size, gate.shape[1]), jnp.float32)
        up_act = jnp.zeros((m * size, gate.shape[1]), jnp.float32)
        for c in range(chunks):
            (de_from(part_of, c) if direct else xd_from(r, c)).wait_recv()
            block = xin[r, c, :, lo : lo + size, :].reshape(m * size, cw)
            gate_act += jnp.dot(block, gate[cols(c), :], preferred_element_type=jnp.float32)
            up_act += jnp.dot(block, up[cols(c), :], preferred_element_type=jnp.float32)
        act = (gate_act / (1.0 + jnp.exp(-gate_act)) * up_act).astype(jnp.bfloat16)
        if opening:
            loads[6].wait()
        for c in range(bchunks):
            made = jnp.dot(act, down[:, bcols(c)], preferred_element_type=jnp.float32)
            res[r, c, :, lo : lo + size, :] = made.astype(jnp.bfloat16).reshape(m, size, bw)
            if send:
                send_back(part_of, c)
            back[r, c, t, lo : lo + size, :] = res[r, c, t, lo : lo + size, :]

    def send_back(part_of, c):
        for j in peers():
            xb_copy(part_of, j, c).start()

    def combined(r, c, i):
        value = jnp.dot(
            mixes[r, :, 0:rows], back[r, c].reshape(rows, bw), preferred_element_type=jnp.float32
        )
        if i is not None:
            value = value + jnp.dot(
                mixes[r, :, rows : 2 * rows], esl[i, c].reshape(rows, bw),
                preferred_element_type=jnp.float32,
            )
        return value

    @pl.when(middle)
    def _():
        pl.semaphore_wait(barrier, 2 * m)
        to_in, to_out = {"ep": inner}, {"ep": outer}
        me_copy(OWN, INNER, 0, to_in).start()
        for c in range(chunks):
            ag_copy(OWN, INNER, 0, c, to_in).start()
        sides = [z, outer]
        select = selection(OWN, sides)
        for c in range(chunks):
            dispatch(OWN, c, select)
        mixing(OWN, sides)

        sel_o = sel_i = None
        for c in range(chunks):
            if c == 0:
                me_copy(OWN, INNER, 0, to_in).wait_recv()
                sel_i = selection(INNER, sides)
            ag_copy(OWN, INNER, 0, c, to_in).wait_recv()
            dispatch(INNER, c, sel_i)
            if c == 0:
                me_copy(OWN, OUTER, 0, to_in).wait_recv()
                me_copy(OUTER, FAR, 1, to_in).start()
                sel_o = selection(OUTER, [z])
            ag_copy(OWN, OUTER, 0, c, to_in).wait_recv()
            ag_copy(OUTER, FAR, 1, c, to_in).start()
            dispatch(OUTER, c, sel_o)
        mixing(INNER, sides)
        experts_step(lot(INNER), False, True)

        me_copy(OUTER, FAR, 1, to_in).wait_recv()
        sel_f = selection(FAR, sides)
        for c in range(chunks):
            ag_copy(OUTER, FAR, 1, c, to_in).wait_recv()
            dispatch(FAR, c, sel_f)
        for c in range(chunks):
            for j in spread():
                de_copy(second_half, j, c).start()
        mixing(FAR, sides)
        mixing(OUTER, [z])
        experts_step(lot(OUTER), False, send=False)

        def to_inner(i, r, c):
            xb_from(lot(r), c).wait_recv()
            es_copy(lot(r), c).wait_recv()
            part[i, c] = combined(r, c, r - 1).astype(jnp.bfloat16)
            rs_copy(i, i, c, to_in).start()

        def to_outer(c):
            xb_from(lot(OUTER), c).wait_recv()
            value = combined(OUTER, c, None)
            rs_copy(1, 1, c, to_in).wait_recv()
            part[2, c] = (value + rin[1, c].astype(jnp.float32)).astype(jnp.bfloat16)
            rs_copy(2, 0, c, to_out).start()

        def finish(c):
            xb_from(lot(OWN), c).wait_recv()
            es_copy(first_half, c).wait_recv()
            es_copy(second_half, c).wait_recv()
            rs_copy(0, 0, c, to_in).wait_recv()
            value = combined(OWN, c, 0) + rin[0, c].astype(jnp.float32)
            out[:, bcols(c)] = value.astype(jnp.bfloat16)

        for c in range(bchunks):
            to_inner(0, INNER, c)
            if c == bchunks // 2 - 1:
                experts_step(lot(FAR), False)
                for d in range(bchunks):
                    send_back(lot(OUTER), d)
        experts_step(lot(OWN), False)
        lag = 3
        for c in range(bchunks + lag):
            if c < bchunks:
                to_inner(1, FAR, c)
            if c >= lag:
                to_outer(c - lag)
        for c in range(bchunks):
            finish(c)

        for s in range(2):
            me_copy(OWN, INNER, s, to_in).wait_send()
            ag_sent(s)
        for part_of in (first_half, lot(INNER), lot(FAR), second_half):
            de_sent(part_of)
        for r in range(4):
            xd_sent(r)
            xb_sent(lot(r))
        for i in range(3):
            rs_sent(i)

    @pl.when(end)
    def _():
        pl.semaphore_wait(barrier, 2 * m - 1)
        to_near = {"ep": near}
        me_copy(OWN, OUTER, 0, to_near).start()
        for c in range(chunks):
            ag_copy(OWN, OUTER, 0, c, to_near).start()
        select = selection(OWN, [z])
        early = chunks // 2
        for c in range(early):
            dispatch(OWN, c, select)
        mixing(OWN, [z])
        lots = [first_half, lot(INNER), lot(FAR), second_half]
        for s, part_of in enumerate(lots):
            experts_step(part_of, True, s == 0)
            if s == 0:
                for c in range(early, chunks):
                    dispatch(OWN, c, select)
            for c in range(bchunks):
                xb_from(part_of, c).wait_recv()
                es_copy(part_of, c).start()
        experts_step(lot(OWN), False)
        for c in range(bchunks):
            xb_from(lot(OWN), c).wait_recv()
            pre[c] = combined(OWN, c, None)
        for c in range(bchunks):
            rs_copy(2, 0, c, to_near).wait_recv()
            value = pre[c] + rin[0, c].astype(jnp.float32)
            out[:, bcols(c)] = value.astype(jnp.bfloat16)

        me_copy(OWN, OUTER, 0, to_near).wait_send()
        ag_sent(0)
        xd_sent(OWN)
        xb_sent(lot(OWN))
        for part_of in lots:
            xb_sent(part_of)
            es_sent(part_of)


def fused(n, m, cap, hidden_in, expert_ids, route_weights, norm_gain, gate_proj, up_proj, down_proj):
    tokens, width = hidden_in.shape
    units = gate_proj.shape[2]
    chunks, bchunks = CHUNKS, BACK_CHUNKS
    choose = expert_ids.shape[1]
    lines = -(-2 * choose // 8) * 8
    bf, f32 = jnp.bfloat16, jnp.float32
    dma = pltpu.SemaphoreType.DMA
    hbm = pl.BlockSpec(memory_space=pltpu.HBM)
    slots = lambda k, q: pltpu.VMEM((k, q, m, cap, width // q), bf)
    block = lambda k, q: pltpu.VMEM((k, q, tokens, width // q), bf)
    return pl.pallas_call(
        functools.partial(kernel, n, m, cap, chunks, bchunks),
        out_shape=jax.ShapeDtypeStruct((tokens, width), bf),
        in_specs=[hbm] * 7,
        out_specs=pl.BlockSpec(memory_space=pltpu.VMEM),
        scratch_shapes=[
            pltpu.VMEM((tokens, width), bf),
            pltpu.VMEM((choose, tokens), jnp.int32),
            pltpu.VMEM((choose, tokens), f32),
            pltpu.VMEM((1, width), f32),
            pltpu.VMEM((width, units), bf),
            pltpu.VMEM((width, units), bf),
            pltpu.VMEM((units, width), bf),
            block(4, chunks),
            pltpu.VMEM((4, lines, tokens), f32),
            pltpu.VMEM((4, tokens, 2 * m * cap), bf),
            slots(4, chunks), slots(3, chunks), slots(4, chunks),
            slots(4, bchunks), slots(4, bchunks), slots(3, bchunks),
            block(3, bchunks), block(2, bchunks),
            pltpu.VMEM((bchunks, tokens, width // bchunks), f32),
            dma((7,)),
            dma((2,)), dma((4, chunks)),
            dma((2,)), dma((4,)),
            dma((4,)), dma((5, chunks)), dma((4,)),
            dma((5,)), dma((5, bchunks)),
            dma((4,)), dma((4, bchunks)),
            dma((3,)), dma((2, bchunks)),
        ],
        compiler_params=pltpu.CompilerParams(
            collective_id=0, has_side_effects=True, vmem_limit_bytes=40 * 1024 * 1024
        ),
        name="experts",
    )(*[
        pltpu.with_memory_space_constraint(array, pltpu.HBM)
        for array in (
            hidden_in, expert_ids.T, route_weights.T, norm_gain.reshape(1, -1),
            gate_proj, up_proj, down_proj,
        )
    ])


def by_slots(capacity, hidden_in, expert_ids, route_weights, norm_gain, gate_proj, up_proj, down_proj):
    token_count = hidden_in.shape[0]
    model_width = hidden_in.shape[1]
    choose_count = expert_ids.shape[1]
    expert_count = lax.axis_size("ep") * lax.axis_size("tp")
    as_float = hidden_in.astype(jnp.float32)
    scaled = as_float * lax.rsqrt(jnp.mean(as_float * as_float, axis=-1, keepdims=True) + 1e-06)
    normed = (scaled * norm_gain).astype(jnp.bfloat16)
    flat_ids = expert_ids.reshape(-1)
    onehot = (flat_ids[:, None] == jnp.arange(expert_count, dtype=jnp.int32)[None, :]).astype(
        jnp.int32
    )
    slot_index = jnp.sum((jnp.cumsum(onehot, axis=0) - onehot) * onehot, axis=1)
    target = flat_ids * capacity + slot_index
    routed = jnp.repeat(normed, choose_count, axis=0)
    buffer = jnp.zeros((expert_count * capacity, model_width), jnp.bfloat16).at[target].set(routed)
    buffer = buffer.reshape(expert_count, capacity, model_width)
    arrived = lax.all_to_all(buffer, ("ep", "tp"), split_axis=0, concat_axis=0, tiled=True)
    shape_in = arrived.shape
    block_in = arrived.reshape(-1, model_width)
    gate_act = jnp.dot(block_in, gate_proj[0], preferred_element_type=jnp.float32)
    up_act = jnp.dot(block_in, up_proj[0], preferred_element_type=jnp.float32)
    hidden = (jax.nn.silu(gate_act) * up_act).astype(jnp.bfloat16)
    result = jnp.dot(hidden, down_proj[0], preferred_element_type=jnp.float32).astype(jnp.bfloat16)
    results = result.reshape(shape_in)
    returned = lax.all_to_all(results, ("ep", "tp"), split_axis=0, concat_axis=0, tiled=True)
    picked = returned.reshape(-1, model_width)[target].astype(jnp.float32)
    picked = picked.reshape(token_count, choose_count, model_width)
    return jnp.sum(picked * route_weights[:, :, None], axis=1).astype(jnp.bfloat16)


def body(hidden_in, expert_ids, *rest):
    n, m = lax.axis_size("ep"), lax.axis_size("tp")
    tokens = hidden_in.shape[0]
    cap = slot_capacity(expert_ids.shape[1], tokens, n * m)
    if n == 4 and m * cap >= tokens and cap % 16 == 0:
        return fused(n, m, cap, hidden_in, expert_ids, *rest)
    return by_slots(cap, hidden_in, expert_ids, *rest)


def solution(mesh):
    return jax.shard_map(
        body,
        mesh=mesh,
        in_specs=(
            P(("grp", "ep", "tp"), None),
            P(("grp", "ep", "tp"), None),
            P(("grp", "ep", "tp"), None),
            P(),
            P(("ep", "tp"), None, None),
            P(("ep", "tp"), None, None),
            P(("ep", "tp"), None, None),
        ),
        out_specs=P(("grp", "ep", "tp"), None),
        check_vma=False,
    )
```

```python
import functools

import jax
import jax.numpy as jnp
from jax import lax
from jax.experimental import pallas as pl
from jax.experimental.pallas import tpu as pltpu
from jax.sharding import PartitionSpec as P

CHUNKS = 4
BACK_CHUNKS = 8
STRAIGHT = (0, 2, 2, 0)
OWN, OUTER, INNER, FAR = 0, 1, 2, 3


def slot_capacity(choose_count, token_count, expert_count):
    return max(2, 2 * choose_count * token_count // expert_count)


def kernel(
    n, m, cap, chunks, bchunks,
    hid_hbm, ids_hbm, wts_hbm, gain_hbm, gate_hbm, up_hbm, down_hbm, out,
    hid, ids, wts, gain, gate, up, down,
    tok, meta, mixes, dsp, dse, xin, res, back, esl, part, rin, pre,
    in_sem, ag_s, ag_r, me_s, me_r, xd_s, xd_r, de_s, xb_s, xb_r, es_s, es_r, rs_s, rs_r,
):
    z = lax.axis_index("ep")
    t = lax.axis_index("tp")
    tokens, width = hid.shape
    rows = m * cap
    cw = width // chunks
    bw = width // bchunks
    half = cap // 2
    choose = ids.shape[0]
    experts = n * m
    middle = jnp.logical_and(z > 0, z < n - 1)
    end = jnp.logical_or(z == 0, z == n - 1)
    inner = n - 1 - z
    outer = jnp.where(z <= 1, 0, n - 1)
    near = jnp.where(z == 0, 1, n - 2)

    def cols(c):
        return pl.ds(c * cw, cw)

    def bcols(c):
        return pl.ds(c * bw, bw)

    loads = [
        pltpu.make_async_copy(src, dst, in_sem.at[i])
        for i, (src, dst) in enumerate([
            (hid_hbm, hid), (ids_hbm, ids), (wts_hbm, wts), (gain_hbm, gain),
            (gate_hbm.at[0], gate), (up_hbm.at[0], up), (down_hbm.at[0], down),
        ])
    ]
    for load in loads:
        load.start()

    barrier = pltpu.get_barrier_semaphore()

    def greet(dev):
        pl.semaphore_signal(
            barrier, inc=1, device_id=dev, device_id_type=pl.DeviceIdType.MESH
        )

    for d in range(1, m):
        greet({"tp": lax.rem(t + d, m)})

    @pl.when(middle)
    def _():
        greet({"ep": inner})
        for j in range(m):
            greet({"ep": outer, "tp": jnp.int32(j)})

    @pl.when(end)
    def _():
        for j in range(m):
            greet({"ep": near, "tp": jnp.int32(j)})

    def remote(src, dst, s_sem, r_sem, dev):
        return pltpu.make_async_remote_copy(
            src_ref=src, dst_ref=dst, send_sem=s_sem, recv_sem=r_sem,
            device_id=dev, device_id_type=pl.DeviceIdType.MESH,
        )

    def lot(r):
        return r, r, 0, cap

    first_half, second_half = (1, 1, 0, half), (4, 1, half, cap - half)
    others, self_id = pl.ds(0, m - 1), {"tp": t}

    def ag_copy(src, dst, slot, c, dev):
        return remote(tok.at[src, c], tok.at[dst, c], ag_s.at[slot], ag_r.at[dst, c], dev)

    def ag_sent(slot):
        remote(tok.at[0], tok.at[0], ag_s.at[slot], ag_r.at[0, 0], self_id).wait_send()

    def me_copy(src, dst, slot, dev):
        return remote(meta.at[src], meta.at[dst], me_s.at[slot], me_r.at[dst], dev)

    def xd_copy(r, j, c):
        return remote(
            dsp.at[r, c, j], xin.at[r, c, t], xd_s.at[r], xd_r.at[r, c], {"tp": j}
        )

    def xd_from(r, c):
        return remote(
            dsp.at[r, c, others], xin.at[r, c, others], xd_s.at[r], xd_r.at[r, c], self_id
        )

    def xd_sent(r):
        remote(
            dsp.at[r, :, others], xin.at[r, :, others], xd_s.at[r], xd_r.at[r, 0], self_id
        ).wait_send()

    def spread():
        return [lax.rem(t + lax.rem(t, 2) + d, m) for d in range(m)]

    def de_copy(part_of, j, c):
        k, r, lo, size = part_of
        here = pl.ds(lo, size)
        return remote(
            dse.at[r - 1, c, j, here], xin.at[r, c, t, here], de_s.at[k - 1],
            xd_r.at[k, c], {"ep": outer, "tp": j},
        )

    def de_from(part_of, c):
        k, r, lo, size = part_of
        here = pl.ds(lo, size)
        return remote(
            dse.at[r - 1, c, :, here], xin.at[r, c, :, here], de_s.at[k - 1],
            xd_r.at[k, c], self_id,
        )

    def de_sent(part_of):
        k, r, lo, size = part_of
        here = pl.ds(lo, size)
        remote(
            dse.at[r - 1, :, :, here], xin.at[r, :, :, here], de_s.at[k - 1],
            xd_r.at[k, 0], self_id,
        ).wait_send()

    def xb_copy(part_of, j, c):
        k, r, lo, size = part_of
        here = pl.ds(lo, size)
        return remote(
            res.at[r, c, j, here], back.at[r, c, t, here], xb_s.at[k],
            xb_r.at[k, c], {"tp": j},
        )

    def xb_from(part_of, c):
        k, r, lo, size = part_of
        here = pl.ds(lo, size)
        return remote(
            res.at[r, c, others, here], back.at[r, c, others, here], xb_s.at[k],
            xb_r.at[k, c], self_id,
        )

    def xb_sent(part_of, skip=0):
        k, r, lo, size = part_of
        here, late = pl.ds(lo, size), pl.ds(skip, bchunks - skip)
        remote(
            res.at[r, late, others, here], back.at[r, late, others, here], xb_s.at[k],
            xb_r.at[k, 0], self_id,
        ).wait_send()

    def st_copy(part_of, j, c):
        k, r, lo, size = part_of
        here = pl.ds(lo, size)
        return remote(
            res.at[r, c, j, here], esl.at[r - 1, c, t, here], es_s.at[k - 1],
            es_r.at[k - 1, c], {"ep": near, "tp": j},
        )

    def es_copy(part_of, c):
        k, r, lo, size = part_of
        here = pl.ds(lo, size)
        return remote(
            back.at[r, c, :, here], esl.at[r - 1, c, :, here], es_s.at[k - 1],
            es_r.at[k - 1, c], {"ep": near},
        )

    def es_sent(part_of):
        k, r, lo, size = part_of
        here = pl.ds(lo, size)
        remote(
            back.at[r, :, :, here], esl.at[r - 1, :, :, here], es_s.at[k - 1],
            es_r.at[k - 1, 0], self_id,
        ).wait_send()

    def rs_copy(i, k, c, dev):
        return remote(part.at[i, c], rin.at[k, c], rs_s.at[i], rs_r.at[k, c], dev)

    def rs_sent(i):
        remote(part.at[i], rin.at[0], rs_s.at[i], rs_r.at[0, 0], self_id).wait_send()

    def peers():
        return [lax.rem(t + d, m) for d in range(m - 1, 0, -1)]

    loads[1].wait()
    loads[2].wait()
    expert_row = lax.broadcasted_iota(jnp.int32, (experts, tokens), 0)
    named = [(expert_row == ids[k : k + 1, :]).astype(jnp.float32) for k in range(choose)]
    total = named[0]
    for k in range(1, choose):
        total = total + named[k]
    before = (
        lax.broadcasted_iota(jnp.int32, (tokens, tokens), 0)
        < lax.broadcasted_iota(jnp.int32, (tokens, tokens), 1)
    ).astype(jnp.bfloat16)
    counts = jnp.dot(total.astype(jnp.bfloat16), before, preferred_element_type=jnp.float32)
    first = expert_row.astype(jnp.float32) * cap + counts
    lines = [jnp.sum(named[k] * first, axis=0, keepdims=True) for k in range(choose)]
    lines += [wts[k : k + 1, :] for k in range(choose)]
    lines.append(jnp.zeros((meta.shape[1] - 2 * choose, tokens), jnp.float32))
    meta[OWN] = jnp.concatenate(lines, axis=0)

    loads[0].wait()
    loads[3].wait()
    hidden = hid[...].astype(jnp.float32)
    scale = lax.rsqrt(jnp.mean(hidden * hidden, axis=-1, keepdims=True) + 1e-06)
    for c in range(chunks):
        normed = hidden[:, c * cw : (c + 1) * cw] * scale * gain[:, cols(c)]
        tok[OWN, c] = normed.astype(jnp.bfloat16)

    def slot_rows(sides):
        parts = [
            lax.broadcasted_iota(jnp.int32, (rows, tokens), 0) + side * rows for side in sides
        ]
        return jnp.concatenate(parts, axis=0).astype(jnp.float32)

    def selection(r, sides):
        info = meta[r]
        row = slot_rows(sides)
        select = jnp.zeros(row.shape, jnp.float32)
        for k in range(choose):
            select = select + (row == info[k : k + 1, :]).astype(jnp.float32)
        return select.astype(jnp.bfloat16)

    def mixing(r, sides):
        info = meta[r]
        row = slot_rows(sides)
        mix = jnp.zeros(row.shape, jnp.float32)
        for k in range(choose):
            mix = mix + jnp.where(
                row == info[k : k + 1, :], info[choose + k : choose + k + 1, :], 0.0
            )
        mixes[r, :, 0 : len(sides) * rows] = jnp.transpose(mix).astype(jnp.bfloat16)

    def dispatch(r, c, select):
        sent = jnp.dot(select, tok[r, c], preferred_element_type=jnp.float32).astype(jnp.bfloat16)
        if select.shape[0] > rows:
            i = 0 if r == OWN else r - 1
            dse[i, c] = sent[rows:, :].reshape(m, cap, cw)
            for j in spread():
                de_copy(first_half if r == OWN else lot(r), j, c).start()
        dsp[r, c] = sent[0:rows, :].reshape(m, cap, cw)
        for j in peers():
            xd_copy(r, j, c).start()
        xin[r, c, t] = dsp[r, c, t]

    def experts_step(part_of, direct, opening=False, send=True, straight=0):
        k, r, lo, size = part_of
        if opening:
            loads[4].wait()
            loads[5].wait()
        gate_act = jnp.zeros((m * size, gate.shape[1]), jnp.float32)
        up_act = jnp.zeros((m * size, gate.shape[1]), jnp.float32)
        for c in range(chunks):
            (de_from(part_of, c) if direct else xd_from(r, c)).wait_recv()
            block = xin[r, c, :, lo : lo + size, :].reshape(m * size, cw)
            gate_act += jnp.dot(block, gate[cols(c), :], preferred_element_type=jnp.float32)
            up_act += jnp.dot(block, up[cols(c), :], preferred_element_type=jnp.float32)
        act = (gate_act / (1.0 + jnp.exp(-gate_act)) * up_act).astype(jnp.bfloat16)
        if opening:
            loads[6].wait()
        for c in range(bchunks):
            made = jnp.dot(act, down[:, bcols(c)], preferred_element_type=jnp.float32)
            res[r, c, :, lo : lo + size, :] = made.astype(jnp.bfloat16).reshape(m, size, bw)
            if c < straight:
                for j in spread():
                    st_copy(part_of, j, c).start()
                continue
            if send:
                send_back(part_of, c)
            back[r, c, t, lo : lo + size, :] = res[r, c, t, lo : lo + size, :]

    def send_back(part_of, c):
        for j in peers():
            xb_copy(part_of, j, c).start()

    def combined(r, c, i):
        value = jnp.dot(
            mixes[r, :, 0:rows], back[r, c].reshape(rows, bw), preferred_element_type=jnp.float32
        )
        if i is not None:
            value = value + jnp.dot(
                mixes[r, :, rows : 2 * rows], esl[i, c].reshape(rows, bw),
                preferred_element_type=jnp.float32,
            )
        return value

    @pl.when(middle)
    def _():
        pl.semaphore_wait(barrier, 2 * m)
        to_in, to_out = {"ep": inner}, {"ep": outer}
        me_copy(OWN, INNER, 0, to_in).start()
        for c in range(chunks):
            ag_copy(OWN, INNER, 0, c, to_in).start()
        sides = [z, outer]
        select = selection(OWN, sides)
        for c in range(chunks):
            dispatch(OWN, c, select)
        mixing(OWN, sides)

        sel_o = sel_i = None
        for c in range(chunks):
            if c == 0:
                me_copy(OWN, INNER, 0, to_in).wait_recv()
                sel_i = selection(INNER, sides)
            ag_copy(OWN, INNER, 0, c, to_in).wait_recv()
            dispatch(INNER, c, sel_i)
            if c == 0:
                me_copy(OWN, OUTER, 0, to_in).wait_recv()
                me_copy(OUTER, FAR, 1, to_in).start()
                sel_o = selection(OUTER, [z])
            ag_copy(OWN, OUTER, 0, c, to_in).wait_recv()
            ag_copy(OUTER, FAR, 1, c, to_in).start()
            dispatch(OUTER, c, sel_o)
        mixing(INNER, sides)
        me_copy(OUTER, FAR, 1, to_in).wait_recv()
        sel_f = selection(FAR, sides)
        for c in range(chunks):
            ag_copy(OUTER, FAR, 1, c, to_in).wait_recv()
            dispatch(FAR, c, sel_f)
            if c == 0:
                experts_step(lot(INNER), False, True)
            if c == 1:
                experts_step(lot(OWN), False, send=False)
        for c in range(chunks):
            for j in spread():
                de_copy(second_half, j, c).start()
        mixing(FAR, sides)
        mixing(OUTER, [z])
        experts_step(lot(OUTER), False, send=False)

        def to_inner(i, r, c):
            xb_from(lot(r), c).wait_recv()
            es_copy(lot(r), c).wait_recv()
            part[i, c] = combined(r, c, r - 1).astype(jnp.bfloat16)
            rs_copy(i, i, c, to_in).start()

        def to_outer(c):
            xb_from(lot(OUTER), c).wait_recv()
            value = combined(OUTER, c, None)
            rs_copy(1, 1, c, to_in).wait_recv()
            part[2, c] = (value + rin[1, c].astype(jnp.float32)).astype(jnp.bfloat16)
            rs_copy(2, 0, c, to_out).start()

        def finish(c):
            xb_from(lot(OWN), c).wait_recv()
            es_copy(first_half, c).wait_recv()
            es_copy(second_half, c).wait_recv()
            rs_copy(0, 0, c, to_in).wait_recv()
            value = combined(OWN, c, 0) + rin[0, c].astype(jnp.float32)
            out[:, bcols(c)] = value.astype(jnp.bfloat16)

        ahead = bchunks // 4
        for c in range(bchunks):
            to_inner(0, INNER, c)
            if c == bchunks // 2:
                for d in range(ahead):
                    send_back(lot(OUTER), d)
            if c == bchunks // 2 + 1:
                experts_step(lot(FAR), False)
                for d in range(ahead, bchunks):
                    send_back(lot(OUTER), d)
                for d in range(bchunks):
                    send_back(lot(OWN), d)
        lag = 3
        for c in range(bchunks + lag):
            if c < bchunks:
                to_inner(1, FAR, c)
            if c >= lag:
                to_outer(c - lag)
        for c in range(bchunks):
            finish(c)

        for s in range(2):
            me_copy(OWN, INNER, s, to_in).wait_send()
            ag_sent(s)
        for part_of in (first_half, lot(INNER), lot(FAR), second_half):
            de_sent(part_of)
        for r in range(4):
            xd_sent(r)
            xb_sent(lot(r))
        for i in range(3):
            rs_sent(i)

    @pl.when(end)
    def _():
        pl.semaphore_wait(barrier, 2 * m - 1)
        to_near = {"ep": near}
        me_copy(OWN, OUTER, 0, to_near).start()
        for c in range(chunks):
            ag_copy(OWN, OUTER, 0, c, to_near).start()
        select = selection(OWN, [z])
        early = chunks // 2
        for c in range(early):
            dispatch(OWN, c, select)
        mixing(OWN, [z])
        lots = [first_half, lot(INNER), lot(FAR), second_half]
        relays = [
            (part_of, c) for k, part_of in enumerate(lots) for c in range(STRAIGHT[k], bchunks)
        ]

        def relay(until):
            while relays and relays[0][0][0] in until:
                part_of, c = relays.pop(0)
                xb_from(part_of, c).wait_recv()
                es_copy(part_of, c).start()
                if part_of[0] == FAR and c == bchunks // 2 - 1:
                    return

        experts_step(first_half, True, True, straight=STRAIGHT[0])
        for c in range(early, chunks):
            dispatch(OWN, c, select)
        relay((1,))
        experts_step(lot(INNER), True, straight=STRAIGHT[1])
        relay((INNER,))
        experts_step(lot(FAR), True, straight=STRAIGHT[2])
        relay((FAR,))
        experts_step(second_half, True, straight=STRAIGHT[3])
        relay((FAR,))
        experts_step(lot(OWN), False)
        relay((4,))
        for c in range(bchunks):
            xb_from(lot(OWN), c).wait_recv()
            pre[c] = combined(OWN, c, None)
        for c in range(bchunks):
            rs_copy(2, 0, c, to_near).wait_recv()
            value = pre[c] + rin[0, c].astype(jnp.float32)
            out[:, bcols(c)] = value.astype(jnp.bfloat16)

        me_copy(OWN, OUTER, 0, to_near).wait_send()
        ag_sent(0)
        xd_sent(OWN)
        xb_sent(lot(OWN))
        for k, part_of in enumerate(lots):
            if STRAIGHT[k] < bchunks:
                xb_sent(part_of, STRAIGHT[k])
            es_sent(part_of)


def fused(n, m, cap, hidden_in, expert_ids, route_weights, norm_gain, gate_proj, up_proj, down_proj):
    tokens, width = hidden_in.shape
    units = gate_proj.shape[2]
    chunks, bchunks = CHUNKS, BACK_CHUNKS
    choose = expert_ids.shape[1]
    lines = -(-2 * choose // 8) * 8
    bf, f32 = jnp.bfloat16, jnp.float32
    dma = pltpu.SemaphoreType.DMA
    hbm = pl.BlockSpec(memory_space=pltpu.HBM)
    slots = lambda k, q: pltpu.VMEM((k, q, m, cap, width // q), bf)
    block = lambda k, q: pltpu.VMEM((k, q, tokens, width // q), bf)
    return pl.pallas_call(
        functools.partial(kernel, n, m, cap, chunks, bchunks),
        out_shape=jax.ShapeDtypeStruct((tokens, width), bf),
        in_specs=[hbm] * 7,
        out_specs=pl.BlockSpec(memory_space=pltpu.VMEM),
        scratch_shapes=[
            pltpu.VMEM((tokens, width), bf),
            pltpu.VMEM((choose, tokens), jnp.int32),
            pltpu.VMEM((choose, tokens), f32),
            pltpu.VMEM((1, width), f32),
            pltpu.VMEM((width, units), bf),
            pltpu.VMEM((width, units), bf),
            pltpu.VMEM((units, width), bf),
            block(4, chunks),
            pltpu.VMEM((4, lines, tokens), f32),
            pltpu.VMEM((4, tokens, 2 * m * cap), bf),
            slots(4, chunks), slots(3, chunks), slots(4, chunks),
            slots(4, bchunks), slots(4, bchunks), slots(3, bchunks),
            block(3, bchunks), block(2, bchunks),
            pltpu.VMEM((bchunks, tokens, width // bchunks), f32),
            dma((7,)),
            dma((2,)), dma((4, chunks)),
            dma((2,)), dma((4,)),
            dma((4,)), dma((5, chunks)), dma((4,)),
            dma((5,)), dma((5, bchunks)),
            dma((4,)), dma((4, bchunks)),
            dma((3,)), dma((2, bchunks)),
        ],
        compiler_params=pltpu.CompilerParams(
            collective_id=0, has_side_effects=True, vmem_limit_bytes=40 * 1024 * 1024
        ),
        name="experts",
    )(*[
        pltpu.with_memory_space_constraint(array, pltpu.HBM)
        for array in (
            hidden_in, expert_ids.T, route_weights.T, norm_gain.reshape(1, -1),
            gate_proj, up_proj, down_proj,
        )
    ])


def by_slots(capacity, hidden_in, expert_ids, route_weights, norm_gain, gate_proj, up_proj, down_proj):
    token_count = hidden_in.shape[0]
    model_width = hidden_in.shape[1]
    choose_count = expert_ids.shape[1]
    expert_count = lax.axis_size("ep") * lax.axis_size("tp")
    as_float = hidden_in.astype(jnp.float32)
    scaled = as_float * lax.rsqrt(jnp.mean(as_float * as_float, axis=-1, keepdims=True) + 1e-06)
    normed = (scaled * norm_gain).astype(jnp.bfloat16)
    flat_ids = expert_ids.reshape(-1)
    onehot = (flat_ids[:, None] == jnp.arange(expert_count, dtype=jnp.int32)[None, :]).astype(
        jnp.int32
    )
    slot_index = jnp.sum((jnp.cumsum(onehot, axis=0) - onehot) * onehot, axis=1)
    target = flat_ids * capacity + slot_index
    routed = jnp.repeat(normed, choose_count, axis=0)
    buffer = jnp.zeros((expert_count * capacity, model_width), jnp.bfloat16).at[target].set(routed)
    buffer = buffer.reshape(expert_count, capacity, model_width)
    arrived = lax.all_to_all(buffer, ("ep", "tp"), split_axis=0, concat_axis=0, tiled=True)
    shape_in = arrived.shape
    block_in = arrived.reshape(-1, model_width)
    gate_act = jnp.dot(block_in, gate_proj[0], preferred_element_type=jnp.float32)
    up_act = jnp.dot(block_in, up_proj[0], preferred_element_type=jnp.float32)
    hidden = (jax.nn.silu(gate_act) * up_act).astype(jnp.bfloat16)
    result = jnp.dot(hidden, down_proj[0], preferred_element_type=jnp.float32).astype(jnp.bfloat16)
    results = result.reshape(shape_in)
    returned = lax.all_to_all(results, ("ep", "tp"), split_axis=0, concat_axis=0, tiled=True)
    picked = returned.reshape(-1, model_width)[target].astype(jnp.float32)
    picked = picked.reshape(token_count, choose_count, model_width)
    return jnp.sum(picked * route_weights[:, :, None], axis=1).astype(jnp.bfloat16)


def body(hidden_in, expert_ids, *rest):
    n, m = lax.axis_size("ep"), lax.axis_size("tp")
    tokens = hidden_in.shape[0]
    cap = slot_capacity(expert_ids.shape[1], tokens, n * m)
    if n == 4 and m * cap >= tokens and cap % 16 == 0:
        return fused(n, m, cap, hidden_in, expert_ids, *rest)
    return by_slots(cap, hidden_in, expert_ids, *rest)


def solution(mesh):
    return jax.shard_map(
        body,
        mesh=mesh,
        in_specs=(
            P(("grp", "ep", "tp"), None),
            P(("grp", "ep", "tp"), None),
            P(("grp", "ep", "tp"), None),
            P(),
            P(("ep", "tp"), None, None),
            P(("ep", "tp"), None, None),
            P(("ep", "tp"), None, None),
        ),
        out_specs=P(("grp", "ep", "tp"), None),
        check_vma=False,
    )
```

```python
import functools

import jax
import jax.numpy as jnp
from jax import lax
from jax.experimental import pallas as pl
from jax.experimental.pallas import tpu as pltpu
from jax.sharding import PartitionSpec as P

CHUNKS = 4
BACK_CHUNKS = 8
STRAIGHT = (0, 2, 2, 0)
OWN, OUTER, INNER, FAR = 0, 1, 2, 3


def slot_capacity(choose_count, token_count, expert_count):
    return max(2, 2 * choose_count * token_count // expert_count)


def kernel(
    n, m, cap, chunks, bchunks,
    hid_hbm, ids_hbm, wts_hbm, gain_hbm, gate_hbm, up_hbm, down_hbm, out,
    hid, ids, wts, gain, gate, up, down,
    tok, meta, mixes, dsp, dse, xin, res, back, esl, part, rin, pre,
    in_sem, ag_s, ag_r, me_s, me_r, xd_s, xd_r, de_s, xb_s, xb_r, es_s, es_r, rs_s, rs_r,
):
    z = lax.axis_index("ep")
    t = lax.axis_index("tp")
    tokens, width = hid.shape
    rows = m * cap
    cw = width // chunks
    bw = width // bchunks
    half = cap // 2
    choose = ids.shape[0]
    experts = n * m
    middle = jnp.logical_and(z > 0, z < n - 1)
    end = jnp.logical_or(z == 0, z == n - 1)
    inner = n - 1 - z
    outer = jnp.where(z <= 1, 0, n - 1)
    near = jnp.where(z == 0, 1, n - 2)

    def cols(c):
        return pl.ds(c * cw, cw)

    def bcols(c):
        return pl.ds(c * bw, bw)

    loads = [
        pltpu.make_async_copy(src, dst, in_sem.at[i])
        for i, (src, dst) in enumerate([
            (hid_hbm, hid), (ids_hbm, ids), (wts_hbm, wts), (gain_hbm, gain),
            (gate_hbm.at[0], gate), (up_hbm.at[0], up), (down_hbm.at[0], down),
        ])
    ]
    for load in loads:
        load.start()

    barrier = pltpu.get_barrier_semaphore()

    def greet(dev):
        pl.semaphore_signal(
            barrier, inc=1, device_id=dev, device_id_type=pl.DeviceIdType.MESH
        )

    for d in range(1, m):
        greet({"tp": lax.rem(t + d, m)})

    @pl.when(middle)
    def _():
        greet({"ep": inner})
        for j in range(m):
            greet({"ep": outer, "tp": jnp.int32(j)})

    @pl.when(end)
    def _():
        for j in range(m):
            greet({"ep": near, "tp": jnp.int32(j)})

    def remote(src, dst, s_sem, r_sem, dev):
        return pltpu.make_async_remote_copy(
            src_ref=src, dst_ref=dst, send_sem=s_sem, recv_sem=r_sem,
            device_id=dev, device_id_type=pl.DeviceIdType.MESH,
        )

    def lot(r):
        return r, r, 0, cap

    first_half, second_half = (1, 1, 0, half), (4, 1, half, cap - half)
    others, self_id = pl.ds(0, m - 1), {"tp": t}

    def ag_copy(src, dst, slot, c, dev):
        return remote(tok.at[src, c], tok.at[dst, c], ag_s.at[slot], ag_r.at[dst, c], dev)

    def ag_sent(slot):
        remote(tok.at[0], tok.at[0], ag_s.at[slot], ag_r.at[0, 0], self_id).wait_send()

    def me_copy(src, dst, slot, dev):
        return remote(meta.at[src], meta.at[dst], me_s.at[slot], me_r.at[dst], dev)

    def xd_copy(r, j, c):
        return remote(
            dsp.at[r, c, j], xin.at[r, c, t], xd_s.at[r], xd_r.at[r, c], {"tp": j}
        )

    def xd_from(r, c):
        return remote(
            dsp.at[r, c, others], xin.at[r, c, others], xd_s.at[r], xd_r.at[r, c], self_id
        )

    def xd_sent(r):
        remote(
            dsp.at[r, :, others], xin.at[r, :, others], xd_s.at[r], xd_r.at[r, 0], self_id
        ).wait_send()

    def spread():
        return [lax.rem(t + lax.rem(t, 2) + d, m) for d in range(m)]

    def de_copy(part_of, j, c):
        k, r, lo, size = part_of
        here = pl.ds(lo, size)
        return remote(
            dse.at[r - 1, c, j, here], xin.at[r, c, t, here], de_s.at[k - 1],
            xd_r.at[k, c], {"ep": outer, "tp": j},
        )

    def de_from(part_of, c):
        k, r, lo, size = part_of
        here = pl.ds(lo, size)
        return remote(
            dse.at[r - 1, c, :, here], xin.at[r, c, :, here], de_s.at[k - 1],
            xd_r.at[k, c], self_id,
        )

    def de_sent(part_of):
        k, r, lo, size = part_of
        here = pl.ds(lo, size)
        remote(
            dse.at[r - 1, :, :, here], xin.at[r, :, :, here], de_s.at[k - 1],
            xd_r.at[k, 0], self_id,
        ).wait_send()

    def xb_copy(part_of, j, c):
        k, r, lo, size = part_of
        here = pl.ds(lo, size)
        return remote(
            res.at[r, c, j, here], back.at[r, c, t, here], xb_s.at[k],
            xb_r.at[k, c], {"tp": j},
        )

    def xb_from(part_of, c):
        k, r, lo, size = part_of
        here = pl.ds(lo, size)
        return remote(
            res.at[r, c, others, here], back.at[r, c, others, here], xb_s.at[k],
            xb_r.at[k, c], self_id,
        )

    def xb_sent(part_of, skip=0):
        k, r, lo, size = part_of
        here, late = pl.ds(lo, size), pl.ds(skip, bchunks - skip)
        remote(
            res.at[r, late, others, here], back.at[r, late, others, here], xb_s.at[k],
            xb_r.at[k, 0], self_id,
        ).wait_send()

    def st_copy(part_of, j, c):
        k, r, lo, size = part_of
        here = pl.ds(lo, size)
        return remote(
            res.at[r, c, j, here], esl.at[r - 1, c, t, here], es_s.at[k - 1],
            es_r.at[k - 1, c], {"ep": near, "tp": j},
        )

    def es_copy(part_of, c):
        k, r, lo, size = part_of
        here = pl.ds(lo, size)
        return remote(
            back.at[r, c, :, here], esl.at[r - 1, c, :, here], es_s.at[k - 1],
            es_r.at[k - 1, c], {"ep": near},
        )

    def es_sent(part_of):
        k, r, lo, size = part_of
        here = pl.ds(lo, size)
        remote(
            back.at[r, :, :, here], esl.at[r - 1, :, :, here], es_s.at[k - 1],
            es_r.at[k - 1, 0], self_id,
        ).wait_send()

    def rs_copy(i, k, c, dev):
        return remote(part.at[i, c], rin.at[k, c], rs_s.at[i], rs_r.at[k, c], dev)

    def rs_sent(i):
        remote(part.at[i], rin.at[0], rs_s.at[i], rs_r.at[0, 0], self_id).wait_send()

    def peers():
        return [lax.rem(t + d, m) for d in range(m - 1, 0, -1)]

    loads[1].wait()
    loads[2].wait()
    expert_row = lax.broadcasted_iota(jnp.int32, (experts, tokens), 0)
    named = [(expert_row == ids[k : k + 1, :]).astype(jnp.float32) for k in range(choose)]
    total = named[0]
    for k in range(1, choose):
        total = total + named[k]
    before = (
        lax.broadcasted_iota(jnp.int32, (tokens, tokens), 0)
        < lax.broadcasted_iota(jnp.int32, (tokens, tokens), 1)
    ).astype(jnp.bfloat16)
    counts = jnp.dot(total.astype(jnp.bfloat16), before, preferred_element_type=jnp.float32)
    first = expert_row.astype(jnp.float32) * cap + counts
    lines = [jnp.sum(named[k] * first, axis=0, keepdims=True) for k in range(choose)]
    lines += [wts[k : k + 1, :] for k in range(choose)]
    lines.append(jnp.zeros((meta.shape[1] - 2 * choose, tokens), jnp.float32))
    meta[OWN] = jnp.concatenate(lines, axis=0)

    loads[0].wait()
    loads[3].wait()
    hidden = hid[...].astype(jnp.float32)
    scale = lax.rsqrt(jnp.mean(hidden * hidden, axis=-1, keepdims=True) + 1e-06)
    for c in range(chunks):
        normed = hidden[:, c * cw : (c + 1) * cw] * scale * gain[:, cols(c)]
        tok[OWN, c] = normed.astype(jnp.bfloat16)

    def slot_rows(sides):
        parts = [
            lax.broadcasted_iota(jnp.int32, (rows, tokens), 0) + side * rows for side in sides
        ]
        return jnp.concatenate(parts, axis=0).astype(jnp.float32)

    def selection(r, sides):
        info = meta[r]
        row = slot_rows(sides)
        select = jnp.zeros(row.shape, jnp.float32)
        for k in range(choose):
            select = select + (row == info[k : k + 1, :]).astype(jnp.float32)
        return select.astype(jnp.bfloat16)

    def mixing(r, sides):
        info = meta[r]
        row = slot_rows(sides)
        mix = jnp.zeros(row.shape, jnp.float32)
        for k in range(choose):
            mix = mix + jnp.where(
                row == info[k : k + 1, :], info[choose + k : choose + k + 1, :], 0.0
            )
        mixes[r, :, 0 : len(sides) * rows] = jnp.transpose(mix).astype(jnp.bfloat16)

    def dispatch(r, c, select):
        sent = jnp.dot(select, tok[r, c], preferred_element_type=jnp.float32).astype(jnp.bfloat16)
        if select.shape[0] > rows:
            i = 0 if r == OWN else r - 1
            dse[i, c] = sent[rows:, :].reshape(m, cap, cw)
            for j in spread():
                de_copy(first_half if r == OWN else lot(r), j, c).start()
        dsp[r, c] = sent[0:rows, :].reshape(m, cap, cw)
        for j in peers():
            xd_copy(r, j, c).start()
        xin[r, c, t] = dsp[r, c, t]

    def experts_step(part_of, direct, opening=False, send=True, straight=0):
        k, r, lo, size = part_of
        if opening:
            loads[4].wait()
            loads[5].wait()
        gate_act = jnp.zeros((m * size, gate.shape[1]), jnp.float32)
        up_act = jnp.zeros((m * size, gate.shape[1]), jnp.float32)
        for c in range(chunks):
            (de_from(part_of, c) if direct else xd_from(r, c)).wait_recv()
            block = xin[r, c, :, lo : lo + size, :].reshape(m * size, cw)
            gate_act += jnp.dot(block, gate[cols(c), :], preferred_element_type=jnp.float32)
            up_act += jnp.dot(block, up[cols(c), :], preferred_element_type=jnp.float32)
        act = (gate_act / (1.0 + jnp.exp(-gate_act)) * up_act).astype(jnp.bfloat16)
        if opening:
            loads[6].wait()
        for c in range(bchunks):
            made = jnp.dot(act, down[:, bcols(c)], preferred_element_type=jnp.float32)
            res[r, c, :, lo : lo + size, :] = made.astype(jnp.bfloat16).reshape(m, size, bw)
            if c < straight:
                for j in spread():
                    st_copy(part_of, j, c).start()
                continue
            if send:
                send_back(part_of, c)
            back[r, c, t, lo : lo + size, :] = res[r, c, t, lo : lo + size, :]

    def send_back(part_of, c):
        for j in peers():
            xb_copy(part_of, j, c).start()

    def combined(r, c, i):
        value = jnp.dot(
            mixes[r, :, 0:rows], back[r, c].reshape(rows, bw), preferred_element_type=jnp.float32
        )
        if i is not None:
            value = value + jnp.dot(
                mixes[r, :, rows : 2 * rows], esl[i, c].reshape(rows, bw),
                preferred_element_type=jnp.float32,
            )
        return value

    @pl.when(middle)
    def _():
        pl.semaphore_wait(barrier, 2 * m)
        to_in, to_out = {"ep": inner}, {"ep": outer}
        me_copy(OWN, INNER, 0, to_in).start()
        for c in range(chunks):
            ag_copy(OWN, INNER, 0, c, to_in).start()
        sides = [z, outer]
        select = selection(OWN, sides)
        for c in range(chunks):
            dispatch(OWN, c, select)
        mixing(OWN, sides)

        sel_o = sel_i = None
        for c in range(chunks):
            if c == 0:
                me_copy(OWN, INNER, 0, to_in).wait_recv()
                sel_i = selection(INNER, sides)
            ag_copy(OWN, INNER, 0, c, to_in).wait_recv()
            dispatch(INNER, c, sel_i)
            if c == 0:
                me_copy(OWN, OUTER, 0, to_in).wait_recv()
                me_copy(OUTER, FAR, 1, to_in).start()
                sel_o = selection(OUTER, [z])
            ag_copy(OWN, OUTER, 0, c, to_in).wait_recv()
            ag_copy(OUTER, FAR, 1, c, to_in).start()
            dispatch(OUTER, c, sel_o)
        mixing(INNER, sides)
        me_copy(OUTER, FAR, 1, to_in).wait_recv()
        sel_f = selection(FAR, sides)
        for c in range(chunks):
            ag_copy(OUTER, FAR, 1, c, to_in).wait_recv()
            dispatch(FAR, c, sel_f)
            if c == 0:
                experts_step(lot(INNER), False, True, send=False)
                for d in range(4):
                    send_back(lot(INNER), d)
            if c == 1:
                experts_step(lot(OWN), False, send=False)
        for c in range(chunks):
            for j in spread():
                de_copy(second_half, j, c).start()
        for d in range(4, bchunks):
            send_back(lot(INNER), d)
        mixing(FAR, sides)
        mixing(OUTER, [z])
        experts_step(lot(OUTER), False, send=False)

        def to_inner(i, r, c):
            xb_from(lot(r), c).wait_recv()
            es_copy(lot(r), c).wait_recv()
            part[i, c] = combined(r, c, r - 1).astype(jnp.bfloat16)
            rs_copy(i, i, c, to_in).start()

        def to_outer(c):
            xb_from(lot(OUTER), c).wait_recv()
            value = combined(OUTER, c, None)
            rs_copy(1, 1, c, to_in).wait_recv()
            part[2, c] = (value + rin[1, c].astype(jnp.float32)).astype(jnp.bfloat16)
            rs_copy(2, 0, c, to_out).start()

        def finish(c):
            xb_from(lot(OWN), c).wait_recv()
            es_copy(first_half, c).wait_recv()
            es_copy(second_half, c).wait_recv()
            rs_copy(0, 0, c, to_in).wait_recv()
            value = combined(OWN, c, 0) + rin[0, c].astype(jnp.float32)
            out[:, bcols(c)] = value.astype(jnp.bfloat16)

        ahead, soon = bchunks // 4, bchunks * 3 // 8
        for c in range(soon):
            if c == soon - 1:
                for d in range(ahead):
                    send_back(lot(OUTER), d)
            to_inner(0, INNER, c)
        experts_step(lot(FAR), False)
        for d in range(ahead, bchunks):
            send_back(lot(OUTER), d)
        for d in range(bchunks):
            send_back(lot(OWN), d)
        late = soon + bchunks * 3 // 8
        for c in range(soon, late):
            to_inner(0, INNER, c)
        lag = 3
        for c in range(bchunks + lag):
            if c < bchunks:
                to_inner(1, FAR, c)
            elif late < bchunks:
                to_inner(0, INNER, late)
                late += 1
            if c >= lag:
                to_outer(c - lag)
        for c in range(late, bchunks):
            to_inner(0, INNER, c)
        for c in range(bchunks):
            finish(c)

        for s in range(2):
            me_copy(OWN, INNER, s, to_in).wait_send()
            ag_sent(s)
        for part_of in (first_half, lot(INNER), lot(FAR), second_half):
            de_sent(part_of)
        for r in range(4):
            xd_sent(r)
            xb_sent(lot(r))
        for i in range(3):
            rs_sent(i)

    @pl.when(end)
    def _():
        pl.semaphore_wait(barrier, 2 * m - 1)
        to_near = {"ep": near}
        me_copy(OWN, OUTER, 0, to_near).start()
        for c in range(chunks):
            ag_copy(OWN, OUTER, 0, c, to_near).start()
        select = selection(OWN, [z])
        early = chunks // 2
        for c in range(early):
            dispatch(OWN, c, select)
        mixing(OWN, [z])
        lots = [first_half, lot(INNER), lot(FAR), second_half]
        def relay(k):
            for c in range(STRAIGHT[k], bchunks):
                xb_from(lots[k], c).wait_recv()
                es_copy(lots[k], c).start()

        experts_step(lots[0], True, True, straight=STRAIGHT[0])
        for c in range(early, chunks):
            dispatch(OWN, c, select)
        relay(0)
        experts_step(lots[1], True, straight=STRAIGHT[1])
        relay(1)
        experts_step(lots[2], True, straight=STRAIGHT[2])
        experts_step(lot(OWN), False, send=False)
        for c in range(bchunks // 2):
            send_back(lot(OWN), c)
        relay(2)
        experts_step(lots[3], True, straight=STRAIGHT[3])
        for c in range(bchunks // 2, bchunks):
            send_back(lot(OWN), c)
        relay(3)
        for c in range(bchunks):
            xb_from(lot(OWN), c).wait_recv()
            pre[c] = combined(OWN, c, None)
        for c in range(bchunks):
            rs_copy(2, 0, c, to_near).wait_recv()
            value = pre[c] + rin[0, c].astype(jnp.float32)
            out[:, bcols(c)] = value.astype(jnp.bfloat16)

        me_copy(OWN, OUTER, 0, to_near).wait_send()
        ag_sent(0)
        xd_sent(OWN)
        xb_sent(lot(OWN))
        for k, part_of in enumerate(lots):
            if STRAIGHT[k] < bchunks:
                xb_sent(part_of, STRAIGHT[k])
            es_sent(part_of)


def fused(n, m, cap, hidden_in, expert_ids, route_weights, norm_gain, gate_proj, up_proj, down_proj):
    tokens, width = hidden_in.shape
    units = gate_proj.shape[2]
    chunks, bchunks = CHUNKS, BACK_CHUNKS
    choose = expert_ids.shape[1]
    lines = -(-2 * choose // 8) * 8
    bf, f32 = jnp.bfloat16, jnp.float32
    dma = pltpu.SemaphoreType.DMA
    hbm = pl.BlockSpec(memory_space=pltpu.HBM)
    slots = lambda k, q: pltpu.VMEM((k, q, m, cap, width // q), bf)
    block = lambda k, q: pltpu.VMEM((k, q, tokens, width // q), bf)
    return pl.pallas_call(
        functools.partial(kernel, n, m, cap, chunks, bchunks),
        out_shape=jax.ShapeDtypeStruct((tokens, width), bf),
        in_specs=[hbm] * 7,
        out_specs=pl.BlockSpec(memory_space=pltpu.VMEM),
        scratch_shapes=[
            pltpu.VMEM((tokens, width), bf),
            pltpu.VMEM((choose, tokens), jnp.int32),
            pltpu.VMEM((choose, tokens), f32),
            pltpu.VMEM((1, width), f32),
            pltpu.VMEM((width, units), bf),
            pltpu.VMEM((width, units), bf),
            pltpu.VMEM((units, width), bf),
            block(4, chunks),
            pltpu.VMEM((4, lines, tokens), f32),
            pltpu.VMEM((4, tokens, 2 * m * cap), bf),
            slots(4, chunks), slots(3, chunks), slots(4, chunks),
            slots(4, bchunks), slots(4, bchunks), slots(3, bchunks),
            block(3, bchunks), block(2, bchunks),
            pltpu.VMEM((bchunks, tokens, width // bchunks), f32),
            dma((7,)),
            dma((2,)), dma((4, chunks)),
            dma((2,)), dma((4,)),
            dma((4,)), dma((5, chunks)), dma((4,)),
            dma((5,)), dma((5, bchunks)),
            dma((4,)), dma((4, bchunks)),
            dma((3,)), dma((2, bchunks)),
        ],
        compiler_params=pltpu.CompilerParams(
            collective_id=0, has_side_effects=True, vmem_limit_bytes=40 * 1024 * 1024
        ),
        name="experts",
    )(*[
        pltpu.with_memory_space_constraint(array, pltpu.HBM)
        for array in (
            hidden_in, expert_ids.T, route_weights.T, norm_gain.reshape(1, -1),
            gate_proj, up_proj, down_proj,
        )
    ])


def by_slots(capacity, hidden_in, expert_ids, route_weights, norm_gain, gate_proj, up_proj, down_proj):
    token_count = hidden_in.shape[0]
    model_width = hidden_in.shape[1]
    choose_count = expert_ids.shape[1]
    expert_count = lax.axis_size("ep") * lax.axis_size("tp")
    as_float = hidden_in.astype(jnp.float32)
    scaled = as_float * lax.rsqrt(jnp.mean(as_float * as_float, axis=-1, keepdims=True) + 1e-06)
    normed = (scaled * norm_gain).astype(jnp.bfloat16)
    flat_ids = expert_ids.reshape(-1)
    onehot = (flat_ids[:, None] == jnp.arange(expert_count, dtype=jnp.int32)[None, :]).astype(
        jnp.int32
    )
    slot_index = jnp.sum((jnp.cumsum(onehot, axis=0) - onehot) * onehot, axis=1)
    target = flat_ids * capacity + slot_index
    routed = jnp.repeat(normed, choose_count, axis=0)
    buffer = jnp.zeros((expert_count * capacity, model_width), jnp.bfloat16).at[target].set(routed)
    buffer = buffer.reshape(expert_count, capacity, model_width)
    arrived = lax.all_to_all(buffer, ("ep", "tp"), split_axis=0, concat_axis=0, tiled=True)
    shape_in = arrived.shape
    block_in = arrived.reshape(-1, model_width)
    gate_act = jnp.dot(block_in, gate_proj[0], preferred_element_type=jnp.float32)
    up_act = jnp.dot(block_in, up_proj[0], preferred_element_type=jnp.float32)
    hidden = (jax.nn.silu(gate_act) * up_act).astype(jnp.bfloat16)
    result = jnp.dot(hidden, down_proj[0], preferred_element_type=jnp.float32).astype(jnp.bfloat16)
    results = result.reshape(shape_in)
    returned = lax.all_to_all(results, ("ep", "tp"), split_axis=0, concat_axis=0, tiled=True)
    picked = returned.reshape(-1, model_width)[target].astype(jnp.float32)
    picked = picked.reshape(token_count, choose_count, model_width)
    return jnp.sum(picked * route_weights[:, :, None], axis=1).astype(jnp.bfloat16)


def body(hidden_in, expert_ids, *rest):
    n, m = lax.axis_size("ep"), lax.axis_size("tp")
    tokens = hidden_in.shape[0]
    cap = slot_capacity(expert_ids.shape[1], tokens, n * m)
    if n == 4 and m * cap >= tokens and cap % 16 == 0:
        return fused(n, m, cap, hidden_in, expert_ids, *rest)
    return by_slots(cap, hidden_in, expert_ids, *rest)


def solution(mesh):
    return jax.shard_map(
        body,
        mesh=mesh,
        in_specs=(
            P(("grp", "ep", "tp"), None),
            P(("grp", "ep", "tp"), None),
            P(("grp", "ep", "tp"), None),
            P(),
            P(("ep", "tp"), None, None),
            P(("ep", "tp"), None, None),
            P(("ep", "tp"), None, None),
        ),
        out_specs=P(("grp", "ep", "tp"), None),
        check_vma=False,
    )
```

```python
import functools

import jax
import jax.numpy as jnp
from jax import lax
from jax.experimental import pallas as pl
from jax.experimental.pallas import tpu as pltpu
from jax.sharding import PartitionSpec as P

CHUNKS = 4
BACK_CHUNKS = 8
STRAIGHT = (0, 2, 2, 0)
OWN, OUTER, INNER, FAR = 0, 1, 2, 3


def slot_capacity(choose_count, token_count, expert_count):
    return max(2, 2 * choose_count * token_count // expert_count)


def kernel(
    n, m, cap, chunks, bchunks,
    hid_hbm, ids_hbm, wts_hbm, gain_hbm, gate_hbm, up_hbm, down_hbm, out,
    hid, ids, wts, gain, gate, up, down,
    tok, meta, mixes, dsp, dse, xin, res, back, esl, part, rin, pre,
    in_sem, ag_s, ag_r, me_s, me_r, xd_s, xd_r, de_s, xb_s, xb_r, es_s, es_r, rs_s, rs_r,
):
    z = lax.axis_index("ep")
    t = lax.axis_index("tp")
    tokens, width = hid.shape
    rows = m * cap
    cw = width // chunks
    bw = width // bchunks
    half = cap // 2
    choose = ids.shape[0]
    experts = n * m
    middle = jnp.logical_and(z > 0, z < n - 1)
    end = jnp.logical_or(z == 0, z == n - 1)
    inner = n - 1 - z
    outer = jnp.where(z <= 1, 0, n - 1)
    near = jnp.where(z == 0, 1, n - 2)

    def cols(c):
        return pl.ds(c * cw, cw)

    def bcols(c):
        return pl.ds(c * bw, bw)

    loads = [
        pltpu.make_async_copy(src, dst, in_sem.at[i])
        for i, (src, dst) in enumerate([
            (hid_hbm, hid), (ids_hbm, ids), (wts_hbm, wts), (gain_hbm, gain),
            (gate_hbm.at[0], gate), (up_hbm.at[0], up), (down_hbm.at[0], down),
        ])
    ]
    for load in loads:
        load.start()

    barrier = pltpu.get_barrier_semaphore()

    def greet(dev):
        pl.semaphore_signal(
            barrier, inc=1, device_id=dev, device_id_type=pl.DeviceIdType.MESH
        )

    for d in range(1, m):
        greet({"tp": lax.rem(t + d, m)})

    @pl.when(middle)
    def _():
        greet({"ep": inner})
        for j in range(m):
            greet({"ep": outer, "tp": jnp.int32(j)})

    @pl.when(end)
    def _():
        for j in range(m):
            greet({"ep": near, "tp": jnp.int32(j)})

    def remote(src, dst, s_sem, r_sem, dev):
        return pltpu.make_async_remote_copy(
            src_ref=src, dst_ref=dst, send_sem=s_sem, recv_sem=r_sem,
            device_id=dev, device_id_type=pl.DeviceIdType.MESH,
        )

    def lot(r):
        return r, r, 0, cap

    first_half, second_half = (1, 1, 0, half), (4, 1, half, cap - half)
    others, self_id = pl.ds(0, m - 1), {"tp": t}

    def ag_copy(src, dst, slot, c, dev):
        return remote(tok.at[src, c], tok.at[dst, c], ag_s.at[slot], ag_r.at[dst, c], dev)

    def ag_sent(slot):
        remote(tok.at[0], tok.at[0], ag_s.at[slot], ag_r.at[0, 0], self_id).wait_send()

    def me_copy(src, dst, slot, dev):
        return remote(meta.at[src], meta.at[dst], me_s.at[slot], me_r.at[dst], dev)

    def xd_copy(r, j, c):
        return remote(
            dsp.at[r, c, j], xin.at[r, c, t], xd_s.at[r], xd_r.at[r, c], {"tp": j}
        )

    def xd_from(r, c):
        return remote(
            dsp.at[r, c, others], xin.at[r, c, others], xd_s.at[r], xd_r.at[r, c], self_id
        )

    def xd_sent(r):
        remote(
            dsp.at[r, :, others], xin.at[r, :, others], xd_s.at[r], xd_r.at[r, 0], self_id
        ).wait_send()

    def spread():
        return [lax.rem(t + lax.rem(t, 2) + d, m) for d in range(m)]

    def de_copy(part_of, j, c):
        k, r, lo, size = part_of
        here = pl.ds(lo, size)
        return remote(
            dse.at[r - 1, c, j, here], xin.at[r, c, t, here], de_s.at[k - 1],
            xd_r.at[k, c], {"ep": outer, "tp": j},
        )

    def de_from(part_of, c):
        k, r, lo, size = part_of
        here = pl.ds(lo, size)
        return remote(
            dse.at[r - 1, c, :, here], xin.at[r, c, :, here], de_s.at[k - 1],
            xd_r.at[k, c], self_id,
        )

    def de_sent(part_of):
        k, r, lo, size = part_of
        here = pl.ds(lo, size)
        remote(
            dse.at[r - 1, :, :, here], xin.at[r, :, :, here], de_s.at[k - 1],
            xd_r.at[k, 0], self_id,
        ).wait_send()

    def xb_copy(part_of, j, c):
        k, r, lo, size = part_of
        here = pl.ds(lo, size)
        return remote(
            res.at[r, c, j, here], back.at[r, c, t, here], xb_s.at[k],
            xb_r.at[k, c], {"tp": j},
        )

    def xb_from(part_of, c):
        k, r, lo, size = part_of
        here = pl.ds(lo, size)
        return remote(
            res.at[r, c, others, here], back.at[r, c, others, here], xb_s.at[k],
            xb_r.at[k, c], self_id,
        )

    def xb_sent(part_of, skip=0):
        k, r, lo, size = part_of
        here, late = pl.ds(lo, size), pl.ds(skip, bchunks - skip)
        remote(
            res.at[r, late, others, here], back.at[r, late, others, here], xb_s.at[k],
            xb_r.at[k, 0], self_id,
        ).wait_send()

    def st_copy(part_of, j, c):
        k, r, lo, size = part_of
        here = pl.ds(lo, size)
        return remote(
            res.at[r, c, j, here], esl.at[r - 1, c, t, here], es_s.at[k - 1],
            es_r.at[k - 1, c], {"ep": near, "tp": j},
        )

    def es_copy(part_of, c):
        k, r, lo, size = part_of
        here = pl.ds(lo, size)
        return remote(
            back.at[r, c, :, here], esl.at[r - 1, c, :, here], es_s.at[k - 1],
            es_r.at[k - 1, c], {"ep": near},
        )

    def es_sent(part_of):
        k, r, lo, size = part_of
        here = pl.ds(lo, size)
        remote(
            back.at[r, :, :, here], esl.at[r - 1, :, :, here], es_s.at[k - 1],
            es_r.at[k - 1, 0], self_id,
        ).wait_send()

    def rs_copy(i, k, c, dev):
        return remote(part.at[i, c], rin.at[k, c], rs_s.at[i], rs_r.at[k, c], dev)

    def rs_half(i, k, h, dev):
        here = pl.ds(h * (tokens // 2), tokens // 2)
        return remote(
            part.at[i, bchunks - 1, here], rin.at[k, bchunks - 1, here], rs_s.at[i],
            rs_r.at[k, bchunks - 1 + h], dev,
        )

    def rs_sent(i):
        remote(part.at[i], rin.at[0], rs_s.at[i], rs_r.at[0, 0], self_id).wait_send()

    def peers():
        return [lax.rem(t + d, m) for d in range(m - 1, 0, -1)]

    loads[1].wait()
    loads[2].wait()
    expert_row = lax.broadcasted_iota(jnp.int32, (experts, tokens), 0)
    named = [(expert_row == ids[k : k + 1, :]).astype(jnp.float32) for k in range(choose)]
    total = named[0]
    for k in range(1, choose):
        total = total + named[k]
    before = (
        lax.broadcasted_iota(jnp.int32, (tokens, tokens), 0)
        < lax.broadcasted_iota(jnp.int32, (tokens, tokens), 1)
    ).astype(jnp.bfloat16)
    counts = jnp.dot(total.astype(jnp.bfloat16), before, preferred_element_type=jnp.float32)
    first = expert_row.astype(jnp.float32) * cap + counts
    lines = [jnp.sum(named[k] * first, axis=0, keepdims=True) for k in range(choose)]
    lines += [wts[k : k + 1, :] for k in range(choose)]
    lines.append(jnp.zeros((meta.shape[1] - 2 * choose, tokens), jnp.float32))
    meta[OWN] = jnp.concatenate(lines, axis=0)

    loads[0].wait()
    loads[3].wait()
    hidden = hid[...].astype(jnp.float32)
    scale = lax.rsqrt(jnp.mean(hidden * hidden, axis=-1, keepdims=True) + 1e-06)
    for c in range(chunks):
        normed = hidden[:, c * cw : (c + 1) * cw] * scale * gain[:, cols(c)]
        tok[OWN, c] = normed.astype(jnp.bfloat16)

    def slot_rows(sides):
        parts = [
            lax.broadcasted_iota(jnp.int32, (rows, tokens), 0) + side * rows for side in sides
        ]
        return jnp.concatenate(parts, axis=0).astype(jnp.float32)

    def selection(r, sides):
        info = meta[r]
        row = slot_rows(sides)
        select = jnp.zeros(row.shape, jnp.float32)
        for k in range(choose):
            select = select + (row == info[k : k + 1, :]).astype(jnp.float32)
        return select.astype(jnp.bfloat16)

    def mixing(r, sides):
        info = meta[r]
        row = slot_rows(sides)
        mix = jnp.zeros(row.shape, jnp.float32)
        for k in range(choose):
            mix = mix + jnp.where(
                row == info[k : k + 1, :], info[choose + k : choose + k + 1, :], 0.0
            )
        mixes[r, :, 0 : len(sides) * rows] = jnp.transpose(mix).astype(jnp.bfloat16)

    def dispatch(r, c, select):
        sent = jnp.dot(select, tok[r, c], preferred_element_type=jnp.float32).astype(jnp.bfloat16)
        if select.shape[0] > rows:
            i = 0 if r == OWN else r - 1
            dse[i, c] = sent[rows:, :].reshape(m, cap, cw)
            for j in spread():
                de_copy(first_half if r == OWN else lot(r), j, c).start()
        dsp[r, c] = sent[0:rows, :].reshape(m, cap, cw)
        for j in peers():
            xd_copy(r, j, c).start()
        xin[r, c, t] = dsp[r, c, t]

    def experts_step(part_of, direct, opening=False, send=True, straight=0):
        k, r, lo, size = part_of
        if opening:
            loads[4].wait()
            loads[5].wait()
        gate_act = jnp.zeros((m * size, gate.shape[1]), jnp.float32)
        up_act = jnp.zeros((m * size, gate.shape[1]), jnp.float32)
        for c in range(chunks):
            (de_from(part_of, c) if direct else xd_from(r, c)).wait_recv()
            block = xin[r, c, :, lo : lo + size, :].reshape(m * size, cw)
            gate_act += jnp.dot(block, gate[cols(c), :], preferred_element_type=jnp.float32)
            up_act += jnp.dot(block, up[cols(c), :], preferred_element_type=jnp.float32)
        act = (gate_act / (1.0 + jnp.exp(-gate_act)) * up_act).astype(jnp.bfloat16)
        if opening:
            loads[6].wait()
        for c in range(bchunks):
            made = jnp.dot(act, down[:, bcols(c)], preferred_element_type=jnp.float32)
            res[r, c, :, lo : lo + size, :] = made.astype(jnp.bfloat16).reshape(m, size, bw)
            if c < straight:
                for j in spread():
                    st_copy(part_of, j, c).start()
                continue
            if send:
                send_back(part_of, c)
            back[r, c, t, lo : lo + size, :] = res[r, c, t, lo : lo + size, :]

    def send_back(part_of, c):
        for j in peers():
            xb_copy(part_of, j, c).start()

    def combined(r, c, i):
        value = jnp.dot(
            mixes[r, :, 0:rows], back[r, c].reshape(rows, bw), preferred_element_type=jnp.float32
        )
        if i is not None:
            value = value + jnp.dot(
                mixes[r, :, rows : 2 * rows], esl[i, c].reshape(rows, bw),
                preferred_element_type=jnp.float32,
            )
        return value

    @pl.when(middle)
    def _():
        pl.semaphore_wait(barrier, 2 * m)
        to_in, to_out = {"ep": inner}, {"ep": outer}
        me_copy(OWN, INNER, 0, to_in).start()
        for c in range(chunks):
            ag_copy(OWN, INNER, 0, c, to_in).start()
        sides = [z, outer]
        select = selection(OWN, sides)
        for c in range(chunks):
            dispatch(OWN, c, select)
        mixing(OWN, sides)

        sel_o = sel_i = None
        for c in range(chunks):
            if c == 0:
                me_copy(OWN, INNER, 0, to_in).wait_recv()
                sel_i = selection(INNER, sides)
            ag_copy(OWN, INNER, 0, c, to_in).wait_recv()
            dispatch(INNER, c, sel_i)
            if c == 0:
                me_copy(OWN, OUTER, 0, to_in).wait_recv()
                me_copy(OUTER, FAR, 1, to_in).start()
                sel_o = selection(OUTER, [z])
            ag_copy(OWN, OUTER, 0, c, to_in).wait_recv()
            ag_copy(OUTER, FAR, 1, c, to_in).start()
            dispatch(OUTER, c, sel_o)
        mixing(INNER, sides)
        me_copy(OUTER, FAR, 1, to_in).wait_recv()
        sel_f = selection(FAR, sides)
        for c in range(chunks):
            ag_copy(OUTER, FAR, 1, c, to_in).wait_recv()
            dispatch(FAR, c, sel_f)
            if c == 0:
                experts_step(lot(INNER), False, True, send=False)
                for d in range(4):
                    send_back(lot(INNER), d)
            if c == 1:
                experts_step(lot(OWN), False, send=False)
        for c in range(chunks):
            for j in spread():
                de_copy(second_half, j, c).start()
        for d in range(4, bchunks):
            send_back(lot(INNER), d)
        mixing(FAR, sides)
        mixing(OUTER, [z])
        experts_step(lot(OUTER), False, send=False)

        def to_inner(i, r, c):
            xb_from(lot(r), c).wait_recv()
            es_copy(lot(r), c).wait_recv()
            part[i, c] = combined(r, c, r - 1).astype(jnp.bfloat16)
            if i == 1 and c == bchunks - 1:
                for h in range(2):
                    rs_half(1, 1, h, to_in).start()
            else:
                rs_copy(i, i, c, to_in).start()

        def to_outer(c):
            xb_from(lot(OUTER), c).wait_recv()
            value = combined(OUTER, c, None)
            if c == bchunks - 1:
                for h in range(2):
                    low, high = h * (tokens // 2), (h + 1) * (tokens // 2)
                    rs_half(1, 1, h, to_in).wait_recv()
                    total = value[low:high] + rin[1, c, low:high].astype(jnp.float32)
                    part[2, c, low:high] = total.astype(jnp.bfloat16)
                    rs_half(2, 0, h, to_out).start()
                return
            rs_copy(1, 1, c, to_in).wait_recv()
            part[2, c] = (value + rin[1, c].astype(jnp.float32)).astype(jnp.bfloat16)
            rs_copy(2, 0, c, to_out).start()

        def finish(c):
            xb_from(lot(OWN), c).wait_recv()
            es_copy(first_half, c).wait_recv()
            es_copy(second_half, c).wait_recv()
            rs_copy(0, 0, c, to_in).wait_recv()
            value = combined(OWN, c, 0) + rin[0, c].astype(jnp.float32)
            out[:, bcols(c)] = value.astype(jnp.bfloat16)

        ahead, soon = bchunks // 4, bchunks * 3 // 8
        for c in range(soon):
            if c == soon - 1:
                for d in range(ahead):
                    send_back(lot(OUTER), d)
            to_inner(0, INNER, c)
        experts_step(lot(FAR), False)
        for d in range(ahead, bchunks):
            send_back(lot(OUTER), d)
        for d in range(bchunks):
            send_back(lot(OWN), d)
        late = soon + bchunks * 3 // 8
        for c in range(soon, late):
            to_inner(0, INNER, c)
        lag = 3
        for c in range(bchunks + lag):
            if c < bchunks:
                to_inner(1, FAR, c)
            elif late < bchunks:
                to_inner(0, INNER, late)
                late += 1
            if c >= lag:
                to_outer(c - lag)
        for c in range(late, bchunks):
            to_inner(0, INNER, c)
        for c in range(bchunks):
            finish(c)

        for s in range(2):
            me_copy(OWN, INNER, s, to_in).wait_send()
            ag_sent(s)
        for part_of in (first_half, lot(INNER), lot(FAR), second_half):
            de_sent(part_of)
        for r in range(4):
            xd_sent(r)
            xb_sent(lot(r))
        for i in range(3):
            rs_sent(i)

    @pl.when(end)
    def _():
        pl.semaphore_wait(barrier, 2 * m - 1)
        to_near = {"ep": near}
        me_copy(OWN, OUTER, 0, to_near).start()
        for c in range(chunks):
            ag_copy(OWN, OUTER, 0, c, to_near).start()
        select = selection(OWN, [z])
        early = chunks // 2
        for c in range(early):
            dispatch(OWN, c, select)
        mixing(OWN, [z])
        lots = [first_half, lot(INNER), lot(FAR), second_half]
        def relay(k):
            for c in range(STRAIGHT[k], bchunks):
                xb_from(lots[k], c).wait_recv()
                es_copy(lots[k], c).start()

        experts_step(lots[0], True, True, straight=STRAIGHT[0])
        for c in range(early, chunks):
            dispatch(OWN, c, select)
        relay(0)
        experts_step(lots[1], True, straight=STRAIGHT[1])
        relay(1)
        experts_step(lots[2], True, straight=STRAIGHT[2])
        experts_step(lot(OWN), False, send=False)
        for c in range(bchunks // 2):
            send_back(lot(OWN), c)
        relay(2)
        experts_step(lots[3], True, straight=STRAIGHT[3])
        for c in range(bchunks // 2, bchunks):
            send_back(lot(OWN), c)
        relay(3)
        for c in range(bchunks):
            xb_from(lot(OWN), c).wait_recv()
            pre[c] = combined(OWN, c, None)
        for c in range(bchunks):
            if c == bchunks - 1:
                for h in range(2):
                    rs_half(2, 0, h, to_near).wait_recv()
            else:
                rs_copy(2, 0, c, to_near).wait_recv()
            value = pre[c] + rin[0, c].astype(jnp.float32)
            out[:, bcols(c)] = value.astype(jnp.bfloat16)

        me_copy(OWN, OUTER, 0, to_near).wait_send()
        ag_sent(0)
        xd_sent(OWN)
        xb_sent(lot(OWN))
        for k, part_of in enumerate(lots):
            if STRAIGHT[k] < bchunks:
                xb_sent(part_of, STRAIGHT[k])
            es_sent(part_of)


def fused(n, m, cap, hidden_in, expert_ids, route_weights, norm_gain, gate_proj, up_proj, down_proj):
    tokens, width = hidden_in.shape
    units = gate_proj.shape[2]
    chunks, bchunks = CHUNKS, BACK_CHUNKS
    choose = expert_ids.shape[1]
    lines = -(-2 * choose // 8) * 8
    bf, f32 = jnp.bfloat16, jnp.float32
    dma = pltpu.SemaphoreType.DMA
    hbm = pl.BlockSpec(memory_space=pltpu.HBM)
    slots = lambda k, q: pltpu.VMEM((k, q, m, cap, width // q), bf)
    block = lambda k, q: pltpu.VMEM((k, q, tokens, width // q), bf)
    return pl.pallas_call(
        functools.partial(kernel, n, m, cap, chunks, bchunks),
        out_shape=jax.ShapeDtypeStruct((tokens, width), bf),
        in_specs=[hbm] * 7,
        out_specs=pl.BlockSpec(memory_space=pltpu.VMEM),
        scratch_shapes=[
            pltpu.VMEM((tokens, width), bf),
            pltpu.VMEM((choose, tokens), jnp.int32),
            pltpu.VMEM((choose, tokens), f32),
            pltpu.VMEM((1, width), f32),
            pltpu.VMEM((width, units), bf),
            pltpu.VMEM((width, units), bf),
            pltpu.VMEM((units, width), bf),
            block(4, chunks),
            pltpu.VMEM((4, lines, tokens), f32),
            pltpu.VMEM((4, tokens, 2 * m * cap), bf),
            slots(4, chunks), slots(3, chunks), slots(4, chunks),
            slots(4, bchunks), slots(4, bchunks), slots(3, bchunks),
            block(3, bchunks), block(2, bchunks),
            pltpu.VMEM((bchunks, tokens, width // bchunks), f32),
            dma((7,)),
            dma((2,)), dma((4, chunks)),
            dma((2,)), dma((4,)),
            dma((4,)), dma((5, chunks)), dma((4,)),
            dma((5,)), dma((5, bchunks)),
            dma((4,)), dma((4, bchunks)),
            dma((3,)), dma((2, bchunks + 1)),
        ],
        compiler_params=pltpu.CompilerParams(
            collective_id=0, has_side_effects=True, vmem_limit_bytes=40 * 1024 * 1024
        ),
        name="experts",
    )(*[
        pltpu.with_memory_space_constraint(array, pltpu.HBM)
        for array in (
            hidden_in, expert_ids.T, route_weights.T, norm_gain.reshape(1, -1),
            gate_proj, up_proj, down_proj,
        )
    ])


def by_slots(capacity, hidden_in, expert_ids, route_weights, norm_gain, gate_proj, up_proj, down_proj):
    token_count = hidden_in.shape[0]
    model_width = hidden_in.shape[1]
    choose_count = expert_ids.shape[1]
    expert_count = lax.axis_size("ep") * lax.axis_size("tp")
    as_float = hidden_in.astype(jnp.float32)
    scaled = as_float * lax.rsqrt(jnp.mean(as_float * as_float, axis=-1, keepdims=True) + 1e-06)
    normed = (scaled * norm_gain).astype(jnp.bfloat16)
    flat_ids = expert_ids.reshape(-1)
    onehot = (flat_ids[:, None] == jnp.arange(expert_count, dtype=jnp.int32)[None, :]).astype(
        jnp.int32
    )
    slot_index = jnp.sum((jnp.cumsum(onehot, axis=0) - onehot) * onehot, axis=1)
    target = flat_ids * capacity + slot_index
    routed = jnp.repeat(normed, choose_count, axis=0)
    buffer = jnp.zeros((expert_count * capacity, model_width), jnp.bfloat16).at[target].set(routed)
    buffer = buffer.reshape(expert_count, capacity, model_width)
    arrived = lax.all_to_all(buffer, ("ep", "tp"), split_axis=0, concat_axis=0, tiled=True)
    shape_in = arrived.shape
    block_in = arrived.reshape(-1, model_width)
    gate_act = jnp.dot(block_in, gate_proj[0], preferred_element_type=jnp.float32)
    up_act = jnp.dot(block_in, up_proj[0], preferred_element_type=jnp.float32)
    hidden = (jax.nn.silu(gate_act) * up_act).astype(jnp.bfloat16)
    result = jnp.dot(hidden, down_proj[0], preferred_element_type=jnp.float32).astype(jnp.bfloat16)
    results = result.reshape(shape_in)
    returned = lax.all_to_all(results, ("ep", "tp"), split_axis=0, concat_axis=0, tiled=True)
    picked = returned.reshape(-1, model_width)[target].astype(jnp.float32)
    picked = picked.reshape(token_count, choose_count, model_width)
    return jnp.sum(picked * route_weights[:, :, None], axis=1).astype(jnp.bfloat16)


def body(hidden_in, expert_ids, *rest):
    n, m = lax.axis_size("ep"), lax.axis_size("tp")
    tokens = hidden_in.shape[0]
    cap = slot_capacity(expert_ids.shape[1], tokens, n * m)
    if n == 4 and m * cap >= tokens and cap % 16 == 0:
        return fused(n, m, cap, hidden_in, expert_ids, *rest)
    return by_slots(cap, hidden_in, expert_ids, *rest)


def solution(mesh):
    return jax.shard_map(
        body,
        mesh=mesh,
        in_specs=(
            P(("grp", "ep", "tp"), None),
            P(("grp", "ep", "tp"), None),
            P(("grp", "ep", "tp"), None),
            P(),
            P(("ep", "tp"), None, None),
            P(("ep", "tp"), None, None),
            P(("ep", "tp"), None, None),
        ),
        out_specs=P(("grp", "ep", "tp"), None),
        check_vma=False,
    )
```
